32 devices in a mesh: ep: 8 (over z, y), tp: 4 (over x, core).
Axes of the slice: x: 2, y: 2, z: 4, core: 2. Of those that a mesh axis runs over, the one named last changes fastest.
Arguments:
- mixer_in: bfloat16 [3072, 2048], P(('ep', 'tp')), may hold values from -6 to 6
- expert_in: bfloat16 [3072, 2048], P(('ep', 'tp')), may hold values from -6 to 6
- mixer_gain: float32 [2048], replicated, may hold values from 0.1 to 1.9
- in_gate_weight: bfloat16 [2048, 2048], P(None, 'tp'), may hold values from -0.125 to 0.125
- out_gate_weight: bfloat16 [2048, 2048], P(None, 'tp'), may hold values from -0.125 to 0.125
- value_weight: bfloat16 [2048, 2048], P(None, 'tp'), may hold values from -0.125 to 0.125
- conv_taps: float32 [3, 2048], replicated, may hold values from -3 to 3
- mixer_proj: bfloat16 [2048, 2048], P(None, 'tp'), may hold values from -0.125 to 0.125
- expert_gain: float32 [2048], replicated, may hold values from 0.1 to 1.9
- route_ids: int32 [3072, 2], P('ep'), may hold values from 0 to 7, all different within a row; in each aligned block of 96 rows (0 to 95, 96 to 191, ...) at most 48 rows name the same one
- route_weights: float32 [3072, 2], P('ep'), may hold values from 0.1 to 1
- gate_weight: bfloat16 [8, 2048, 1024], P('ep', None, 'tp'), may hold values from -0.125 to 0.125
- up_weight: bfloat16 [8, 2048, 1024], P('ep', None, 'tp'), may hold values from -0.125 to 0.125
- down_weight: bfloat16 [8, 1024, 2048], P('ep', None, 'tp'), may hold values from -0.1875 to 0.1875
Outputs:
- mixer_out: bfloat16 [3072, 2048], P('ep', 'tp')
- expert_out: bfloat16 [3072, 2048], P('ep', 'tp')
The draws below stay inside these ranges and needn't reach their ends.
Inputs may be any that keep to these rules, and one draw needn't show every extreme that they name: `route_ids`: each row names 2 different experts. In each aligned block of 96 rows no expert is named by more than 48 rows, a bound that some block reaches.
All inputs are finite; a program needn't handle non-finite values.
Results may differ from the reference program's by a relative error of at most 0.0076.
Values may be sent and summed in bfloat16 or wider, within the bound.
No kernel may reach another device: no remote copies, remote signals or barrier semaphores. Data moves between devices by JAX's collectives and lax.ppermute only.
A program may use at most 64 MiB of HBM per device.

```python
import math
import jax
import jax.numpy as jnp
import numpy as np
from jax import lax

D = 2048
F = 1024
CONV = 3
TOP_K = 2
TOK_DEV = 96
EXPERTS = 8
CAPQ = 48
TOKENS = 3072
N_EP = 8
N_TP = 4


def shard_levels(rng, extent, pieces, low, high):
    def one(position, blocks):
        draws = jax.random.uniform(jax.random.fold_in(jax.random.fold_in(rng, 6), position), (blocks,), jnp.float32, low / len(pieces), high / len(pieces))
        return jnp.repeat(jnp.exp(draws), extent[position] // blocks).reshape((-1,) + (1,) * (len(extent) - position - 1))

    level = one(*pieces[0])
    for cut in pieces[1:]:
        level = level * one(*cut)
    return level


def routed_block(own_key, own, number, rows, amount, top, limit, slope):
    order = jax.random.permutation(own_key, amount)
    heavy_load, common = portions_of(amount, rows * top, limit, slope, True), portions_of(amount, rows * top, limit, slope, False)
    places = jnp.arange(amount)

    def named(lengths, rotation):
        used = int((lengths > 0).sum())
        fixed = max(1, used // 4)
        passed = fixed + (places - fixed + rotation * (used - fixed)) % max(1, amount - fixed)
        return jnp.zeros((amount,), jnp.int32).at[order[jnp.where(places < fixed, places, passed)]].set(jnp.asarray(lengths, jnp.int32))

    lengths = jnp.where(number % 4 == 0, named(heavy_load, number // 4), named(common, number - number // 4 - 1))
    mixed = jax.random.permutation(jax.random.fold_in(own, 3), amount)
    donor, receiver = mixed[0:amount // 2 * 2:2], mixed[1:amount // 2 * 2:2]
    margin = jnp.minimum(lengths[donor] - 1, limit - lengths[receiver]) // 2
    margin = jnp.where((donor == order[0]) | (receiver == order[0]) | (lengths[receiver] == 0), 0, jnp.maximum(margin, 0))
    passed = jax.random.randint(jax.random.fold_in(own, 4), (amount // 2,), 0, 1 << 20) % (margin + 1)
    lengths = lengths.at[donor].add(-passed).at[receiver].add(passed)
    items = jnp.searchsorted(jnp.cumsum(lengths), jnp.arange(rows * top), side="right").astype(jnp.int32)
    table = items.reshape(top, rows).T
    table = table[jax.random.permutation(jax.random.fold_in(own, 1), rows)]
    rotation = jax.random.randint(jax.random.fold_in(own, 2), (rows, 1), 0, top)
    return jnp.take_along_axis(table, (jnp.arange(top)[None, :] + rotation) % top, axis=1)


def portions_of(count, total, most, skew, full):
    loads = [(1 << 20) // math.isqrt(standing ** skew) + 1 for standing in range(1, count + 1)]
    largest = most if full else min(most, max(-(-total // count), total * loads[0] // sum(loads)))
    least = 1 if total - largest >= count - 1 else 0
    given, surplus = [largest] + [least] * (count - 1), total - largest - least * (count - 1)
    while surplus > 0:
        candidates = [i for i in range(1, count) if given[i] < largest] or [i for i in range(1, count) if given[i] < most]
        mass, left = sum([loads[i] for i in candidates]), surplus
        for i in candidates:
            extra = min(most - given[i], max(1, left * loads[i] // mass), surplus)
            given[i] = given[i] + extra
            surplus = surplus - extra
    return np.array(given)


def centred(stream_key, dims, width, limit, pieces=(), held_as=jnp.bfloat16):
    loudness = shard_levels(stream_key, dims, pieces, -0.22, 0.18) if pieces else 1.0
    entries = jax.random.normal(stream_key, dims, jnp.float32) * width * loudness
    return jnp.minimum(jnp.maximum(entries, -limit), limit).astype(held_as)


def setup_inputs(seed: int = 0) -> dict:
    key_of = jax.random.split(jax.random.key(seed), 15)
    mixer_in = centred(key_of[0], (TOKENS, D), 1.0, 6.0, ((0, 32),))
    expert_in = centred(key_of[1], (TOKENS, D), 1.0, 6.0, ((0, 32),))
    mixer_gain = jnp.clip(1.0 + 0.18 * jax.random.normal(key_of[2], (D,), jnp.float32), 0.1, 1.9)
    in_gate_weight = centred(key_of[3], (D, D), D ** -0.5, 0.125, ((1, 4),))
    out_gate_weight = centred(key_of[4], (D, D), D ** -0.5, 0.125, ((1, 4),))
    value_weight = centred(key_of[5], (D, D), D ** -0.5, 0.125, ((1, 4),))
    conv_taps = centred(key_of[6], (CONV, D), 0.577, 3.0, (), jnp.float32)
    mixer_proj = centred(key_of[7], (D, D), D ** -0.5, 0.125, ((1, 4),))
    expert_gain = jnp.clip(1.0 + 0.18 * jax.random.normal(key_of[8], (D,), jnp.float32), 0.1, 1.9)
    route_ids_keys = jax.random.split(jax.random.fold_in(key_of[9], 1), TOKENS // TOK_DEV)
    route_ids_turns = jax.random.permutation(jax.random.fold_in(key_of[9], 3), TOKENS // TOK_DEV)
    route_ids = jax.vmap(lambda own, number: routed_block(jax.random.fold_in(key_of[9], 2), own, number, TOK_DEV, EXPERTS, TOP_K, CAPQ, 1))(route_ids_keys, route_ids_turns).reshape((TOKENS, TOP_K))
    route_weights = jnp.clip(jnp.exp(math.log(1.0) - 2.3025851 * jax.random.uniform(key_of[10], (TOKENS, TOP_K), jnp.float32) ** shard_levels(key_of[10], (TOKENS, TOP_K), ((0, 8),), -0.2, 0.2)), 0.1, 1.0)
    gate_weight = centred(key_of[11], (EXPERTS, D, F), D ** -0.5, 0.125, ((0, 8), (2, 4)))
    up_weight = centred(key_of[12], (EXPERTS, D, F), D ** -0.5, 0.125, ((0, 8), (2, 4)))
    down_weight = centred(key_of[13], (EXPERTS, F, D), F ** -0.5, 0.1875, ((0, 8), (2, 4)))
    return dict(mixer_in=mixer_in, expert_in=expert_in, mixer_gain=mixer_gain, in_gate_weight=in_gate_weight, out_gate_weight=out_gate_weight, value_weight=value_weight, conv_taps=conv_taps, mixer_proj=mixer_proj, expert_gain=expert_gain, route_ids=route_ids, route_weights=route_weights, gate_weight=gate_weight, up_weight=up_weight, down_weight=down_weight)


norm_eps = 1e-06

def rms_rows(values, gain_row):
    wide = values.astype(jnp.float32)
    scale = lax.rsqrt(lax.optimization_barrier(jnp.mean(wide * wide, axis=-1, keepdims=True)) + norm_eps)
    return (wide * scale * gain_row.astype(jnp.float32)).astype(jnp.bfloat16)

def place_slots(route_ids, group_rows, experts, slot_cap):
    row_total, top_count = route_ids.shape
    groups = row_total // group_rows
    labels = jnp.arange(experts, dtype=jnp.int32)
    onehot = (route_ids.reshape(groups, group_rows * top_count)[:, :, None] == labels[None, None, :]).astype(jnp.int32)
    earlier = jnp.cumsum(onehot, axis=1) - onehot
    within = lax.optimization_barrier(jnp.sum(earlier * onehot, axis=2))
    slot_index = jnp.arange(groups, dtype=jnp.int32)[:, None] * slot_cap + within
    return slot_index.reshape(row_total, top_count).astype(jnp.int32)

def reference(mixer_in, expert_in, mixer_gain, in_gate_weight, out_gate_weight, value_weight, conv_taps, mixer_proj, expert_gain, route_ids, route_weights, gate_weight, up_weight, down_weight):
    mixer_normed = rms_rows(mixer_in, mixer_gain)
    in_gate = jnp.dot(mixer_normed, in_gate_weight, preferred_element_type=jnp.float32)
    out_gate = jnp.dot(mixer_normed, out_gate_weight, preferred_element_type=jnp.float32)
    values = jnp.dot(mixer_normed, value_weight, preferred_element_type=jnp.float32)
    product = (in_gate * values).astype(jnp.bfloat16)
    product = lax.optimization_barrier(product)
    row_count = product.shape[0]
    tap_count = conv_taps.shape[0]
    padded = jnp.pad(product.astype(jnp.float32), ((tap_count - 1, 0), (0, 0)))
    tap_rows = conv_taps.astype(jnp.float32)
    conv_sum = tap_rows[0] * padded[0:row_count]
    for tap_index in range(1, tap_count):
        conv_sum = conv_sum + tap_rows[tap_index] * padded[tap_index:tap_index + row_count]
    gated = (out_gate * conv_sum).astype(jnp.bfloat16)
    mixer_out = jnp.dot(gated, mixer_proj, preferred_element_type=jnp.float32).astype(jnp.bfloat16)
    expert_normed = rms_rows(expert_in, expert_gain)
    token_count = expert_normed.shape[0]
    top_count = route_ids.shape[1]
    per_expert = N_EP * N_TP * CAPQ
    slot_index = place_slots(route_ids, TOK_DEV, EXPERTS, CAPQ)
    flat_index = (route_ids * per_expert + slot_index).reshape(-1)
    shares = (route_weights / lax.optimization_barrier(jnp.sum(route_weights, axis=1, keepdims=True))).reshape(-1)
    row_table = jnp.full((EXPERTS * per_expert,), token_count, jnp.int32).at[flat_index].set(jnp.repeat(jnp.arange(token_count, dtype=jnp.int32), top_count))
    share_table = jnp.zeros((EXPERTS * per_expert,), jnp.float32).at[flat_index].set(shares)
    padded_rows = jnp.concatenate([expert_normed, jnp.zeros((1, expert_normed.shape[1]), jnp.bfloat16)], axis=0)

    def one_expert(running, expert_idx):
        rows_here = lax.dynamic_slice_in_dim(row_table, expert_idx * per_expert, per_expert)
        share_here = lax.dynamic_slice_in_dim(share_table, expert_idx * per_expert, per_expert)
        chosen = padded_rows[rows_here]
        gate_pre = jnp.dot(chosen, gate_weight[expert_idx], preferred_element_type=jnp.float32)
        up_pre = jnp.dot(chosen, up_weight[expert_idx], preferred_element_type=jnp.float32)
        hidden = (jax.nn.silu(gate_pre) * up_pre).astype(jnp.bfloat16)
        result = jnp.dot(hidden, down_weight[expert_idx], preferred_element_type=jnp.float32).astype(jnp.bfloat16)
        running = running.at[rows_here].add(share_here[:, None] * result.astype(jnp.float32))
        return (running, None)
    running, _ = lax.scan(one_expert, jnp.zeros((token_count + 1, expert_normed.shape[1]), jnp.float32), jnp.arange(EXPERTS, dtype=jnp.int32))
    expert_out = running[:token_count].astype(jnp.bfloat16)
    return (mixer_out, expert_out)
```

```python
import jax
import jax.numpy as jnp
from jax import lax
from jax.sharding import PartitionSpec as P

norm_eps = 1e-06


def rms_rows(values, gain_row):
    wide = values.astype(jnp.float32)
    scale = lax.rsqrt(jnp.mean(wide * wide, axis=-1, keepdims=True) + norm_eps)
    return (wide * scale * gain_row).astype(jnp.bfloat16)


def swapped(value, axis, mask):
    count = lax.axis_size(axis)
    return lax.ppermute(value, axis, [(source, source ^ mask) for source in range(count)])


def after(value, *earlier):
    return lax.optimization_barrier((value,) + earlier)[0]


def slot_masks(block_ids, labels, slot_cap):
    rows = block_ids.shape[1]
    hits = block_ids[:, None, :] == labels[None, :, None]
    member = jnp.any(hits, axis=0)
    order = jnp.arange(rows, dtype=jnp.int32)
    before = (order[:, None] < order[None, :]).astype(jnp.bfloat16)
    rank = jnp.dot(member.astype(jnp.bfloat16), before, preferred_element_type=jnp.float32)
    rank = jnp.where(member, rank, -1.0)
    slots = jnp.arange(slot_cap, dtype=jnp.int32).astype(jnp.float32)
    return hits, rank[:, None, :] == slots[None, :, None]


def exchange(chunks, axis, direct):
    if direct:
        return [chunks[0]] + [swapped(chunks[k], axis, k) for k in range(1, chunks.shape[0])]
    moved = lax.all_to_all(chunks, axis, split_axis=0, concat_axis=0, tiled=True)
    return [moved.reshape(-1, chunks.shape[2])]


def combine_rows(mask, hits, share_rows, returned):
    share_of = jnp.sum(jnp.where(hits, share_rows[:, None, :], 0.0), axis=0)
    mixed = jnp.where(mask, share_of[:, None, :], 0.0).reshape(-1, mask.shape[2])
    high = mixed.astype(jnp.bfloat16)
    low = (mixed - high.astype(jnp.float32)).astype(jnp.bfloat16)
    dims = (((0,), (0,)), ((), ()))
    total = lax.dot_general(high, returned, dims, preferred_element_type=jnp.float32)
    total = total + lax.dot_general(low, returned, dims, preferred_element_type=jnp.float32)
    return total.astype(jnp.bfloat16)


def on_device(
    mixer_in,
    expert_in,
    mixer_gain,
    in_gate_weight,
    out_gate_weight,
    value_weight,
    conv_taps,
    mixer_proj,
    expert_gain,
    route_ids,
    route_weights,
    gate_weight,
    up_weight,
    down_weight,
):
    tok_dev = mixer_in.shape[0]
    tp_count = lax.axis_size("tp")
    ep_count = lax.axis_size("ep")
    top_count = route_ids.shape[1]
    experts = ep_count * gate_weight.shape[0]
    slot_cap = max(2, 2 * tok_dev * top_count // experts)
    tp_index = lax.axis_index("tp")
    ep_index = lax.axis_index("ep")
    direct = ep_count <= 16 and ep_count & (ep_count - 1) == 0
    near, far = 1, tp_count // 2

    gates, ups = {0: gate_weight[0]}, {0: up_weight[0]}
    gates[far] = swapped(gates[0], "tp", far)
    ups[far] = swapped(ups[0], "tp", far)
    gates[near] = swapped(gates[0], "tp", near)
    ups[near] = swapped(ups[0], "tp", near)
    gates[far ^ near] = swapped(gates[far], "tp", near)
    ups[far ^ near] = swapped(ups[far], "tp", near)
    down_own = down_weight[0]
    down_near = swapped(down_own, "tp", near)
    order = [0, near, far, far ^ near]
    hid_width = gates[0].shape[1]

    def rows_of(weight, j, width):
        return lax.dynamic_slice_in_dim(weight, (tp_index ^ j) * width, width, 0)

    down_all = jnp.concatenate(
        [
            jnp.concatenate([rows_of(down_own, j, hid_width) for j in order], axis=0),
            jnp.concatenate([rows_of(down_near, j, hid_width) for j in order], axis=0),
        ],
        axis=1,
    )

    peers = jnp.arange(experts, dtype=jnp.int32)
    labels = (peers ^ ep_index) if direct else peers

    def block_of(values, j):
        return lax.dynamic_slice_in_dim(values, (tp_index ^ j) * tok_dev, tok_dev, 0)

    hits_own, mask_own = slot_masks(block_of(route_ids, 0).T, labels, slot_cap)
    hits_far, mask_far = slot_masks(block_of(route_ids, far).T, labels, slot_cap)
    expert_normed = rms_rows(expert_in, expert_gain)
    outgoing = jnp.dot(
        mask_own.reshape(-1, tok_dev).astype(jnp.bfloat16),
        expert_normed,
        preferred_element_type=jnp.float32,
    ).astype(jnp.bfloat16)
    outgoing = outgoing.reshape(experts, slot_cap, -1)
    slots_in = jnp.concatenate(exchange(outgoing, "ep", direct), axis=0)

    hidden = {}
    for j in order:
        gate_pre = jnp.dot(slots_in, gates[j], preferred_element_type=jnp.float32)
        up_pre = jnp.dot(slots_in, ups[j], preferred_element_type=jnp.float32)
        hidden[j] = (jax.nn.silu(gate_pre) * up_pre).astype(jnp.bfloat16)
    hidden_own = jnp.concatenate([hidden[j] for j in order], axis=1)
    hidden_sent = jnp.concatenate([hidden[j ^ far] for j in order], axis=1)
    hidden_far = swapped(hidden_sent, "tp", far)

    def results_of(hidden_rows):
        done = jnp.dot(hidden_rows, down_all, preferred_element_type=jnp.float32)
        chunks = done.astype(jnp.bfloat16).reshape(experts, slot_cap, -1)
        return jnp.concatenate(exchange(chunks, "ep", direct), axis=0)

    shares = route_weights / jnp.sum(route_weights, axis=1, keepdims=True)
    mixed_own = combine_rows(mask_own, hits_own, block_of(shares, 0).T, results_of(hidden_own))
    mixed_far = combine_rows(mask_far, hits_far, block_of(shares, far).T, results_of(hidden_far))
    mixed = jnp.concatenate([mixed_own, mixed_far], axis=0)
    col_width = down_own.shape[1]
    mixed_near = swapped(mixed[:, col_width:], "tp", near)
    expert_out = jnp.zeros((tp_count * tok_dev, col_width), jnp.bfloat16)
    for j, block in (
        (0, mixed[:tok_dev, :col_width]),
        (far, mixed[tok_dev:, :col_width]),
        (near, mixed_near[:tok_dev]),
        (far ^ near, mixed_near[tok_dev:]),
    ):
        expert_out = lax.dynamic_update_slice_in_dim(
            expert_out, block, (tp_index ^ j) * tok_dev, 0
        )

    normed = {0: after(rms_rows(mixer_in, mixer_gain), ups[far])}
    normed[far] = swapped(normed[0], "tp", far)
    normed[near] = swapped(normed[0], "tp", near)
    normed[far ^ near] = swapped(normed[far], "tp", near)
    mixer_rows = jnp.zeros((tp_count * tok_dev, mixer_in.shape[1]), jnp.bfloat16)
    for j in order:
        mixer_rows = lax.dynamic_update_slice_in_dim(
            mixer_rows, normed[j], (tp_index ^ j) * tok_dev, 0
        )
    chan_width = in_gate_weight.shape[1]
    in_gate = jnp.dot(mixer_rows, in_gate_weight, preferred_element_type=jnp.float32)
    out_gate = jnp.dot(mixer_rows, out_gate_weight, preferred_element_type=jnp.float32)
    values = jnp.dot(mixer_rows, value_weight, preferred_element_type=jnp.float32)
    product = (in_gate * values).astype(jnp.bfloat16)
    tap_count = conv_taps.shape[0]
    row_count = product.shape[0]
    rim_rows = lax.ppermute(
        product[row_count - (tap_count - 1) :], "ep", [(i, i + 1) for i in range(ep_count - 1)]
    )
    extended = jnp.concatenate([rim_rows, product], axis=0).astype(jnp.float32)
    tap_rows = lax.dynamic_slice_in_dim(conv_taps, tp_index * chan_width, chan_width, 1)
    conv_sum = tap_rows[0] * extended[0:row_count]
    for tap_index in range(1, tap_count):
        conv_sum = conv_sum + tap_rows[tap_index] * extended[tap_index : tap_index + row_count]
    gated = {0: (out_gate * conv_sum).astype(jnp.bfloat16)}
    gated[far] = swapped(gated[0], "tp", far)
    gated[near] = swapped(gated[0], "tp", near)
    gated[far ^ near] = swapped(gated[far], "tp", near)
    mixer_sum = None
    for j in order:
        term = jnp.dot(
            gated[j], rows_of(mixer_proj, j, chan_width), preferred_element_type=jnp.float32
        )
        mixer_sum = term if mixer_sum is None else mixer_sum + term
    return (mixer_sum.astype(jnp.bfloat16), expert_out)


def solution(mesh):
    return jax.shard_map(
        on_device,
        mesh=mesh,
        in_specs=(
            P(("ep", "tp"), None),
            P(("ep", "tp"), None),
            P(),
            P(None, "tp"),
            P(None, "tp"),
            P(None, "tp"),
            P(),
            P(None, "tp"),
            P(),
            P("ep", None),
            P("ep", None),
            P("ep", None, "tp"),
            P("ep", None, "tp"),
            P("ep", None, "tp"),
        ),
        out_specs=(P("ep", "tp"), P("ep", "tp")),
        check_vma=False,
    )
```

```python
import functools

import jax
import jax.numpy as jnp
from jax import lax
from jax.experimental import pallas as pl
from jax.experimental.pallas import tpu as pltpu
from jax.sharding import PartitionSpec as P

norm_eps = 1e-06


def rms_rows(values, gain_row):
    wide = values.astype(jnp.float32)
    scale = lax.rsqrt(jnp.mean(wide * wide, axis=-1, keepdims=True) + norm_eps)
    return (wide * scale * gain_row).astype(jnp.bfloat16)


def swapped(value, axis, mask):
    count = lax.axis_size(axis)
    return lax.ppermute(value, axis, [(source, source ^ mask) for source in range(count)])


def after(value, *earlier):
    return lax.optimization_barrier((value,) + earlier)[0]


def slot_masks(block_ids, labels, slot_cap):
    rows = block_ids.shape[1]
    hits = block_ids[:, None, :] == labels[None, :, None]
    member = jnp.any(hits, axis=0)
    order = jnp.arange(rows, dtype=jnp.int32)
    before = (order[:, None] < order[None, :]).astype(jnp.bfloat16)
    rank = jnp.dot(member.astype(jnp.bfloat16), before, preferred_element_type=jnp.float32)
    rank = jnp.where(member, rank, -1.0)
    slots = jnp.arange(slot_cap, dtype=jnp.int32).astype(jnp.float32)
    return hits, rank[:, None, :] == slots[None, :, None]


def exchange(chunks, axis, direct):
    if direct:
        return [chunks[0]] + [swapped(chunks[k], axis, k) for k in range(1, len(chunks))]
    (rows,) = chunks
    split = rows.reshape(lax.axis_size(axis), -1, rows.shape[1])
    moved = lax.all_to_all(split, axis, split_axis=0, concat_axis=0, tiled=True)
    return [moved.reshape(rows.shape)]


MIB = 1 << 20
ANY = pl.BlockSpec(memory_space=pl.ANY)
VMEM = pl.BlockSpec(memory_space=pltpu.VMEM)
SMEM = pl.BlockSpec(memory_space=pltpu.SMEM)


def dispatch_kernel(direct, slot_cap, place_ref, ids_ref, rows_ref, gain_ref, *out_refs):
    tok, width = rows_ref.shape
    total = ids_ref.shape[1]
    slots = sum(ref.shape[0] for ref in out_refs)
    experts = slots // slot_cap
    lanes = min(total, -(-tok // 128) * 128)
    tp_index, ep_index = place_ref[0], place_ref[1]
    ids = pltpu.roll(ids_ref[...], lax.rem(total - tp_index * tok, total), 1)[:, :lanes]
    labels = lax.broadcasted_iota(jnp.int32, (experts, lanes), 0)
    if direct:
        labels = labels ^ ep_index
    member = ids[0:1] == labels
    for pick in range(1, ids_ref.shape[0]):
        member = member | (ids[pick : pick + 1] == labels)
    first = lax.broadcasted_iota(jnp.int32, (lanes, lanes), 0)
    second = lax.broadcasted_iota(jnp.int32, (lanes, lanes), 1)
    before = jnp.where(first < second, 1.0, 0.0).astype(jnp.bfloat16)
    member = jnp.where(member, 1.0, 0.0)
    rank = jnp.dot(member.astype(jnp.bfloat16), before, preferred_element_type=jnp.float32)
    rank = jnp.where(member > 0.5, rank, -1.0).astype(jnp.bfloat16)
    slot = lax.broadcasted_iota(jnp.int32, (slots, experts), 0)
    start = lax.broadcasted_iota(jnp.int32, (slots, experts), 1) * slot_cap
    inside = (slot >= start) & (slot < start + slot_cap)
    spread = jnp.where(inside, 1.0, 0.0)
    rank_of = jnp.dot(spread.astype(jnp.bfloat16), rank, preferred_element_type=jnp.float32)
    offset = jnp.where(inside, (slot - start).astype(jnp.float32), 0.0)
    offset = jnp.sum(offset, axis=1, keepdims=True)
    mask = jnp.where(rank_of == offset, 1.0, 0.0)[:, :tok].astype(jnp.bfloat16)
    wide = rows_ref[...].astype(jnp.float32)
    scale = lax.rsqrt(jnp.mean(wide * wide, axis=-1, keepdims=True) + norm_eps)
    normed = (wide * scale * gain_ref[...]).astype(jnp.bfloat16)
    step = min(width, 512)
    for col in range(0, width, step):
        part = jnp.dot(mask, normed[:, col : col + step], preferred_element_type=jnp.float32)
        part = part.astype(jnp.bfloat16)
        row = 0
        for ref in out_refs:
            ref[:, col : col + step] = part[row : row + ref.shape[0]]
            row += ref.shape[0]


def dispatched(place, ids, rows, gain, sizes, direct, slot_cap):
    width = rows.shape[1]
    return pl.pallas_call(
        functools.partial(dispatch_kernel, direct, slot_cap),
        out_shape=[jax.ShapeDtypeStruct((size, width), jnp.bfloat16) for size in sizes],
        in_specs=[SMEM, VMEM, VMEM, VMEM],
        out_specs=[VMEM] * len(sizes),
        compiler_params=pltpu.CompilerParams(vmem_limit_bytes=12 * MIB),
        cost_estimate=pl.CostEstimate(
            flops=2 * sum(sizes) * rows.shape[0] * width, bytes_accessed=2 * MIB, transcendentals=0
        ),
        name="dispatch",
    )(place, ids, rows, gain)


def hidden_kernel(row_count, pair_count, *refs):
    row_refs, refs = refs[:row_count], refs[row_count:]
    weight_refs, refs = refs[: 2 * pair_count], refs[2 * pair_count :]
    out_ref, rows, weights, row_sems, weight_sems = refs
    copies, row = [], 0
    for index, ref in enumerate(row_refs):
        target = rows.at[pl.ds(row, ref.shape[0])]
        copies.append(pltpu.make_async_copy(ref, target, row_sems.at[index]))
        row += ref.shape[0]
    loads = [
        pltpu.make_async_copy(ref, weights.at[index], weight_sems.at[index])
        for index, ref in enumerate(weight_refs)
    ]
    for copy in copies + loads:
        copy.start()
    for copy in copies:
        copy.wait()
    width = weights.shape[2]
    for pair in range(pair_count):
        loads[2 * pair].wait()
        gate_pre = jnp.dot(rows[...], weights[2 * pair], preferred_element_type=jnp.float32)
        loads[2 * pair + 1].wait()
        up_pre = jnp.dot(rows[...], weights[2 * pair + 1], preferred_element_type=jnp.float32)
        hidden = gate_pre / (1.0 + jnp.exp(-gate_pre)) * up_pre
        out_ref[:, pair * width : (pair + 1) * width] = hidden.astype(jnp.bfloat16)


def hidden_of(row_parts, pairs):
    rows = sum(part.shape[0] for part in row_parts)
    depth, width = pairs[0][0].shape
    weights = [weight for pair in pairs for weight in pair]
    return pl.pallas_call(
        functools.partial(hidden_kernel, len(row_parts), len(pairs)),
        out_shape=jax.ShapeDtypeStruct((rows, width * len(pairs)), jnp.bfloat16),
        in_specs=[ANY] * (len(row_parts) + len(weights)),
        out_specs=VMEM,
        scratch_shapes=[
            pltpu.VMEM((rows, depth), jnp.bfloat16),
            pltpu.VMEM((len(weights), depth, width), jnp.bfloat16),
            pltpu.SemaphoreType.DMA((len(row_parts),)),
            pltpu.SemaphoreType.DMA((len(weights),)),
        ],
        compiler_params=pltpu.CompilerParams(vmem_limit_bytes=16 * MIB),
        cost_estimate=pl.CostEstimate(
            flops=2 * rows * depth * width * len(weights),
            bytes_accessed=2 * (rows * depth + len(weights) * depth * width),
            transcendentals=rows * width * len(pairs),
        ),
        name="hidden",
    )(*row_parts, *weights)


def down_kernel(base, place_ref, first_ref, second_ref, own_ref, near_ref, *out_refs):
    half = first_ref.shape[1] // 2
    col = 0
    for weight_ref in (own_ref, near_ref):
        total = None
        for j in range(4):
            source = first_ref if j < 2 else second_ref
            block = source[:, (j % 2) * half : (j % 2 + 1) * half]
            start = pl.multiple_of((place_ref[0] ^ base ^ j) * half, half)
            term = jnp.dot(
                block, weight_ref[pl.ds(start, half), :], preferred_element_type=jnp.float32
            )
            total = term if total is None else total + term
        total = total.astype(jnp.bfloat16)
        row = 0
        for ref in out_refs:
            ref[:, col : col + total.shape[1]] = total[row : row + ref.shape[0]]
            row += ref.shape[0]
        col += total.shape[1]


def results_of(place, base, first, second, down_own, down_near, sizes):
    width = 2 * down_own.shape[1]
    return pl.pallas_call(
        functools.partial(down_kernel, base),
        out_shape=[jax.ShapeDtypeStruct((size, width), jnp.bfloat16) for size in sizes],
        in_specs=[SMEM, VMEM, VMEM, VMEM, VMEM],
        out_specs=[VMEM] * len(sizes),
        compiler_params=pltpu.CompilerParams(vmem_limit_bytes=12 * MIB),
        cost_estimate=pl.CostEstimate(
            flops=2 * sum(sizes) * down_own.shape[0] * width,
            bytes_accessed=4 * MIB,
            transcendentals=0,
        ),
        name="down",
    )(place, first, second, down_own, down_near)


def combine_rows(mask, hits, share_rows, returned):
    share_of = jnp.sum(jnp.where(hits, share_rows[:, None, :], 0.0), axis=0)
    mixed = jnp.where(mask, share_of[:, None, :], 0.0).reshape(-1, mask.shape[2])
    high = mixed.astype(jnp.bfloat16)
    low = (mixed - high.astype(jnp.float32)).astype(jnp.bfloat16)
    dims = (((0,), (0,)), ((), ()))
    total = lax.dot_general(high, returned, dims, preferred_element_type=jnp.float32)
    total = total + lax.dot_general(low, returned, dims, preferred_element_type=jnp.float32)
    return total.astype(jnp.bfloat16)


def on_device(
    mixer_in,
    expert_in,
    mixer_gain,
    in_gate_weight,
    out_gate_weight,
    value_weight,
    conv_taps,
    mixer_proj,
    expert_gain,
    route_ids,
    route_weights,
    gate_weight,
    up_weight,
    down_weight,
):
    tok_dev = mixer_in.shape[0]
    tp_count = lax.axis_size("tp")
    ep_count = lax.axis_size("ep")
    top_count = route_ids.shape[1]
    experts = ep_count * gate_weight.shape[0]
    slot_cap = max(2, 2 * tok_dev * top_count // experts)
    tp_index = lax.axis_index("tp")
    ep_index = lax.axis_index("ep")
    direct = ep_count <= 16 and ep_count & (ep_count - 1) == 0
    near, far = 1, tp_count // 2

    gates, ups = {0: gate_weight[0]}, {0: up_weight[0]}
    gates[far] = swapped(gates[0], "tp", far)
    ups[far] = swapped(ups[0], "tp", far)
    gates[near] = swapped(gates[0], "tp", near)
    ups[near] = swapped(ups[0], "tp", near)
    gates[far ^ near] = swapped(gates[far], "tp", near)
    ups[far ^ near] = swapped(ups[far], "tp", near)
    down_own = down_weight[0]
    down_near = swapped(down_own, "tp", near)
    order = [0, near, far, far ^ near]

    def rows_of(weight, j, width):
        return lax.dynamic_slice_in_dim(weight, (tp_index ^ j) * width, width, 0)

    peers = jnp.arange(experts, dtype=jnp.int32)
    labels = (peers ^ ep_index) if direct else peers

    def block_of(values, j):
        return lax.dynamic_slice_in_dim(values, (tp_index ^ j) * tok_dev, tok_dev, 0)

    hits_own, mask_own = slot_masks(block_of(route_ids, 0).T, labels, slot_cap)
    hits_far, mask_far = slot_masks(block_of(route_ids, far).T, labels, slot_cap)
    place = jnp.where(jnp.arange(2) == 0, tp_index, ep_index).astype(jnp.int32)
    sizes = [slot_cap] * experts if direct else [experts * slot_cap]
    outgoing = dispatched(
        place, route_ids.T, expert_in, expert_gain[None, :], sizes, direct, slot_cap
    )
    slots_in = exchange(outgoing, "ep", direct)

    first = hidden_of(slots_in, [(gates[j], ups[j]) for j in (0, near)])
    second = hidden_of(slots_in, [(gates[j], ups[j]) for j in (far, far ^ near)])
    first_far = swapped(after(first, ups[far]), "tp", far)
    second_far = swapped(second, "tp", far)

    def returned(base, one, two):
        done = results_of(place, base, one, two, down_own, down_near, sizes)
        return jnp.concatenate(exchange(done, "ep", direct), axis=0)

    shares = route_weights / jnp.sum(route_weights, axis=1, keepdims=True)
    mixed_own = combine_rows(mask_own, hits_own, block_of(shares, 0).T, returned(0, first, second))
    mixed_far = combine_rows(mask_far, hits_far, block_of(shares, far).T, returned(far, first_far, second_far))
    mixed = jnp.concatenate([mixed_own, mixed_far], axis=0)
    col_width = down_own.shape[1]
    mixed_near = swapped(mixed[:, col_width:], "tp", near)
    expert_out = jnp.zeros((tp_count * tok_dev, col_width), jnp.bfloat16)
    for j, block in (
        (0, mixed[:tok_dev, :col_width]),
        (far, mixed[tok_dev:, :col_width]),
        (near, mixed_near[:tok_dev]),
        (far ^ near, mixed_near[tok_dev:]),
    ):
        expert_out = lax.dynamic_update_slice_in_dim(
            expert_out, block, (tp_index ^ j) * tok_dev, 0
        )

    normed = {0: after(rms_rows(mixer_in, mixer_gain), ups[far])}
    normed[far] = swapped(normed[0], "tp", far)
    normed[near] = swapped(normed[0], "tp", near)
    normed[far ^ near] = swapped(normed[far], "tp", near)
    mixer_rows = jnp.zeros((tp_count * tok_dev, mixer_in.shape[1]), jnp.bfloat16)
    for j in order:
        mixer_rows = lax.dynamic_update_slice_in_dim(
            mixer_rows, normed[j], (tp_index ^ j) * tok_dev, 0
        )
    chan_width = in_gate_weight.shape[1]
    in_gate = jnp.dot(mixer_rows, in_gate_weight, preferred_element_type=jnp.float32)
    out_gate = jnp.dot(mixer_rows, out_gate_weight, preferred_element_type=jnp.float32)
    values = jnp.dot(mixer_rows, value_weight, preferred_element_type=jnp.float32)
    product = (in_gate * values).astype(jnp.bfloat16)
    tap_count = conv_taps.shape[0]
    row_count = product.shape[0]
    rim_rows = lax.ppermute(
        product[row_count - (tap_count - 1) :], "ep", [(i, i + 1) for i in range(ep_count - 1)]
    )
    extended = jnp.concatenate([rim_rows, product], axis=0).astype(jnp.float32)
    tap_rows = lax.dynamic_slice_in_dim(conv_taps, tp_index * chan_width, chan_width, 1)
    conv_sum = tap_rows[0] * extended[0:row_count]
    for tap_index in range(1, tap_count):
        conv_sum = conv_sum + tap_rows[tap_index] * extended[tap_index : tap_index + row_count]
    gated = {0: (out_gate * conv_sum).astype(jnp.bfloat16)}
    gated[far] = swapped(gated[0], "tp", far)
    gated[near] = swapped(gated[0], "tp", near)
    gated[far ^ near] = swapped(gated[far], "tp", near)
    mixer_sum = None
    for j in order:
        term = jnp.dot(
            gated[j], rows_of(mixer_proj, j, chan_width), preferred_element_type=jnp.float32
        )
        mixer_sum = term if mixer_sum is None else mixer_sum + term
    return (mixer_sum.astype(jnp.bfloat16), expert_out)


def solution(mesh):
    return jax.shard_map(
        on_device,
        mesh=mesh,
        in_specs=(
            P(("ep", "tp"), None),
            P(("ep", "tp"), None),
            P(),
            P(None, "tp"),
            P(None, "tp"),
            P(None, "tp"),
            P(),
            P(None, "tp"),
            P(),
            P("ep", None),
            P("ep", None),
            P("ep", None, "tp"),
            P("ep", None, "tp"),
            P("ep", None, "tp"),
        ),
        out_specs=(P("ep", "tp"), P("ep", "tp")),
        check_vma=False,
    )
```

```python
import functools

import jax
import jax.numpy as jnp
from jax import lax
from jax.experimental import pallas as pl
from jax.experimental.pallas import tpu as pltpu
from jax.sharding import PartitionSpec as P


norm_eps = 1e-06


def rms_rows(values, gain_row):
    wide = values.astype(jnp.float32)
    scale = lax.rsqrt(jnp.mean(wide * wide, axis=-1, keepdims=True) + norm_eps)
    return (wide * scale * gain_row).astype(jnp.bfloat16)


def swapped(value, axis, mask):
    count = lax.axis_size(axis)
    return lax.ppermute(value, axis, [(source, source ^ mask) for source in range(count)])


def after(value, *earlier):
    return lax.optimization_barrier((value,) + earlier)[0]


def slot_masks(block_ids, labels, slot_cap):
    rows = block_ids.shape[1]
    hits = block_ids[:, None, :] == labels[None, :, None]
    member = jnp.any(hits, axis=0)
    order = jnp.arange(rows, dtype=jnp.int32)
    before = (order[:, None] < order[None, :]).astype(jnp.bfloat16)
    rank = jnp.dot(member.astype(jnp.bfloat16), before, preferred_element_type=jnp.float32)
    rank = jnp.where(member, rank, -1.0)
    slots = jnp.arange(slot_cap, dtype=jnp.int32).astype(jnp.float32)
    return hits, rank[:, None, :] == slots[None, :, None]


def swaps_direct(count):
    return count <= 16 and count & (count - 1) == 0


def far_first(count):
    return sorted(range(1, count), key=lambda k: (-k.bit_length(), k))


def exchange(chunks, axis, direct):
    if direct:
        moved = {0: chunks[0]}
        for k in far_first(len(chunks)):
            moved[k] = swapped(chunks[k], axis, k)
        return [moved[k] for k in range(len(chunks))]
    (rows,) = chunks
    split = rows.reshape(lax.axis_size(axis), -1, rows.shape[1])
    moved = lax.all_to_all(split, axis, split_axis=0, concat_axis=0, tiled=True)
    return [moved.reshape(rows.shape)]


MIB = 1 << 20
HBM = pl.BlockSpec(memory_space=pltpu.HBM)
VMEM = pl.BlockSpec(memory_space=pltpu.VMEM)
SMEM = pl.BlockSpec(memory_space=pltpu.SMEM)


def dispatch_kernel(direct, slot_cap, place_ref, ids_ref, source_ref, gain_ref, *refs):
    out_refs, (rows_ref, sem) = refs[:-2], refs[-2:]
    load = pltpu.make_async_copy(source_ref, rows_ref, sem)
    load.start()
    tok, width = rows_ref.shape
    total = ids_ref.shape[1]
    slots = sum(ref.shape[0] for ref in out_refs)
    experts = slots // slot_cap
    lanes = min(total, -(-tok // 128) * 128)
    tp_index, ep_index = place_ref[0], place_ref[1]
    ids = pltpu.roll(ids_ref[...], lax.rem(total - tp_index * tok, total), 1)[:, :lanes]
    labels = lax.broadcasted_iota(jnp.int32, (experts, lanes), 0)
    if direct:
        labels = labels ^ ep_index
    member = ids[0:1] == labels
    for pick in range(1, ids_ref.shape[0]):
        member = member | (ids[pick : pick + 1] == labels)
    first = lax.broadcasted_iota(jnp.int32, (lanes, lanes), 0)
    second = lax.broadcasted_iota(jnp.int32, (lanes, lanes), 1)
    before = jnp.where(first < second, 1.0, 0.0).astype(jnp.bfloat16)
    member = jnp.where(member, 1.0, 0.0)
    rank = jnp.dot(member.astype(jnp.bfloat16), before, preferred_element_type=jnp.float32)
    rank = jnp.where(member > 0.5, rank, -1.0).astype(jnp.bfloat16)
    slot = lax.broadcasted_iota(jnp.int32, (slots, experts), 0)
    start = lax.broadcasted_iota(jnp.int32, (slots, experts), 1) * slot_cap
    inside = (slot >= start) & (slot < start + slot_cap)
    spread = jnp.where(inside, 1.0, 0.0)
    rank_of = jnp.dot(spread.astype(jnp.bfloat16), rank, preferred_element_type=jnp.float32)
    offset = jnp.where(inside, (slot - start).astype(jnp.float32), 0.0)
    offset = jnp.sum(offset, axis=1, keepdims=True)
    mask = jnp.where(rank_of == offset, 1.0, 0.0)[:, :tok].astype(jnp.bfloat16)
    load.wait()
    wide = rows_ref[...].astype(jnp.float32)
    scale = lax.rsqrt(jnp.mean(wide * wide, axis=-1, keepdims=True) + norm_eps)
    normed = (wide * scale * gain_ref[...]).astype(jnp.bfloat16)
    step = min(width, 512)
    for col in range(0, width, step):
        part = jnp.dot(mask, normed[:, col : col + step], preferred_element_type=jnp.float32)
        part = part.astype(jnp.bfloat16)
        row = 0
        for ref in out_refs:
            ref[:, col : col + step] = part[row : row + ref.shape[0]]
            row += ref.shape[0]


def dispatched(place, ids, rows, gain, sizes, direct, slot_cap):
    width = rows.shape[1]
    return pl.pallas_call(
        functools.partial(dispatch_kernel, direct, slot_cap),
        out_shape=[jax.ShapeDtypeStruct((size, width), jnp.bfloat16) for size in sizes],
        in_specs=[SMEM, VMEM, HBM, VMEM],
        out_specs=[VMEM] * len(sizes),
        scratch_shapes=[pltpu.VMEM(rows.shape, rows.dtype), pltpu.SemaphoreType.DMA],
        compiler_params=pltpu.CompilerParams(vmem_limit_bytes=56 * MIB),
        cost_estimate=pl.CostEstimate(
            flops=2 * sum(sizes) * rows.shape[0] * width, bytes_accessed=2 * MIB, transcendentals=0
        ),
        name="dispatch",
    )(place, ids, rows, gain)


def hidden_kernel(row_count, *refs):
    row_refs, refs = refs[:row_count], refs[row_count:]
    weight_refs, (out_ref, rows, weights, row_sems, weight_sems) = refs[:-5], refs[-5:]
    copies, row = [], 0
    for index, ref in enumerate(row_refs):
        target = rows.at[pl.ds(row, ref.shape[0])]
        copies.append(pltpu.make_async_copy(ref, target, row_sems.at[index]))
        row += ref.shape[0]
    loads = []
    for index, ref in enumerate(weight_refs):
        width = ref.shape[1]
        target = weights.at[index % 2, :, pl.ds(index // 2 * width, width)]
        loads.append(pltpu.make_async_copy(ref, target, weight_sems.at[index]))
    for copy in copies + loads[0::2] + loads[1::2]:
        copy.start()
    for copy in copies + loads[0::2]:
        copy.wait()
    gate_pre = jnp.dot(rows[...], weights[0], preferred_element_type=jnp.float32)
    for load in loads[1::2]:
        load.wait()
    up_pre = jnp.dot(rows[...], weights[1], preferred_element_type=jnp.float32)
    out_ref[...] = (gate_pre / (1.0 + jnp.exp(-gate_pre)) * up_pre).astype(jnp.bfloat16)


def hidden_of(row_parts, pairs):
    rows = sum(part.shape[0] for part in row_parts)
    depth, width = pairs[0][0].shape
    weights = [weight for pair in pairs for weight in pair]
    return pl.pallas_call(
        functools.partial(hidden_kernel, len(row_parts)),
        out_shape=jax.ShapeDtypeStruct((rows, width * len(pairs)), jnp.bfloat16),
        in_specs=[HBM] * (len(row_parts) + len(weights)),
        out_specs=VMEM,
        scratch_shapes=[
            pltpu.VMEM((rows, depth), jnp.bfloat16),
            pltpu.VMEM((2, depth, width * len(pairs)), jnp.bfloat16),
            pltpu.SemaphoreType.DMA((len(row_parts),)),
            pltpu.SemaphoreType.DMA((len(weights),)),
        ],
        compiler_params=pltpu.CompilerParams(vmem_limit_bytes=56 * MIB),
        cost_estimate=pl.CostEstimate(
            flops=2 * rows * depth * width * len(weights),
            bytes_accessed=2 * (rows * depth + len(weights) * depth * width),
            transcendentals=rows * width * len(pairs),
        ),
        name="hidden",
    )(*row_parts, *weights)


def down_kernel(base, place_ref, first_ref, second_ref, own_ref, near_ref, *out_refs):
    half = first_ref.shape[1] // 2
    col = 0
    for weight_ref in (own_ref, near_ref):
        total = None
        for j in range(4):
            source = first_ref if j < 2 else second_ref
            block = source[:, (j % 2) * half : (j % 2 + 1) * half]
            start = pl.multiple_of((place_ref[0] ^ base ^ j) * half, half)
            term = jnp.dot(
                block, weight_ref[pl.ds(start, half), :], preferred_element_type=jnp.float32
            )
            total = term if total is None else total + term
        total = total.astype(jnp.bfloat16)
        row = 0
        for ref in out_refs:
            ref[:, col : col + total.shape[1]] = total[row : row + ref.shape[0]]
            row += ref.shape[0]
        col += total.shape[1]


def results_of(place, base, first, second, down_own, down_near, sizes):
    width = 2 * down_own.shape[1]
    return pl.pallas_call(
        functools.partial(down_kernel, base),
        out_shape=[jax.ShapeDtypeStruct((size, width), jnp.bfloat16) for size in sizes],
        in_specs=[SMEM, VMEM, VMEM, VMEM, VMEM],
        out_specs=[VMEM] * len(sizes),
        compiler_params=pltpu.CompilerParams(vmem_limit_bytes=12 * MIB),
        cost_estimate=pl.CostEstimate(
            flops=2 * sum(sizes) * down_own.shape[0] * width,
            bytes_accessed=4 * MIB,
            transcendentals=0,
        ),
        name="down",
    )(place, first, second, down_own, down_near)


def combine_rows(mask, hits, share_rows, returned):
    share_of = jnp.sum(jnp.where(hits, share_rows[:, None, :], 0.0), axis=0)
    mixed = jnp.where(mask, share_of[:, None, :], 0.0).reshape(-1, mask.shape[2])
    high = mixed.astype(jnp.bfloat16)
    low = (mixed - high.astype(jnp.float32)).astype(jnp.bfloat16)
    dims = (((0,), (0,)), ((), ()))
    total = lax.dot_general(high, returned, dims, preferred_element_type=jnp.float32)
    total = total + lax.dot_general(low, returned, dims, preferred_element_type=jnp.float32)
    return total.astype(jnp.bfloat16)


def on_device(
    mixer_in,
    expert_in,
    mixer_gain,
    in_gate_weight,
    out_gate_weight,
    value_weight,
    conv_taps,
    mixer_proj,
    expert_gain,
    route_ids,
    route_weights,
    gate_weight,
    up_weight,
    down_weight,
):
    tok_dev = mixer_in.shape[0]
    tp_count = lax.axis_size("tp")
    ep_count = lax.axis_size("ep")
    top_count = route_ids.shape[1]
    experts = ep_count * gate_weight.shape[0]
    slot_cap = max(2, 2 * tok_dev * top_count // experts)
    tp_index = lax.axis_index("tp")
    ep_index = lax.axis_index("ep")
    direct = swaps_direct(ep_count)
    near, far = 1, tp_count // 2

    gates, ups = {0: gate_weight[0]}, {0: up_weight[0]}
    gates[far] = swapped(gates[0], "tp", far)
    ups[far] = swapped(ups[0], "tp", far)
    gates[near] = swapped(gates[0], "tp", near)
    ups[near] = swapped(ups[0], "tp", near)
    down_own = down_weight[0]
    down_near = swapped(down_own, "tp", near)
    order = [0, near, far, far ^ near]

    def rows_of(weight, j, width):
        return lax.dynamic_slice_in_dim(weight, (tp_index ^ j) * width, width, 0)

    peers = jnp.arange(experts, dtype=jnp.int32)
    labels = (peers ^ ep_index) if direct else peers

    def block_of(values, j):
        return lax.dynamic_slice_in_dim(values, (tp_index ^ j) * tok_dev, tok_dev, 0)

    hits_own, mask_own = slot_masks(block_of(route_ids, 0).T, labels, slot_cap)
    hits_far, mask_far = slot_masks(block_of(route_ids, far).T, labels, slot_cap)
    place = jnp.where(jnp.arange(2) == 0, tp_index, ep_index).astype(jnp.int32)
    sizes = [slot_cap] * experts if direct else [experts * slot_cap]
    outgoing = dispatched(
        place, route_ids.T, expert_in, expert_gain[None, :], sizes, direct, slot_cap
    )
    slots_in = exchange(outgoing, "ep", direct)

    first = hidden_of(slots_in, [(gates[j], ups[j]) for j in (0, near)])
    gates[far ^ near] = swapped(after(gates[far], first), "tp", near)
    ups[far ^ near] = swapped(after(ups[far], first), "tp", near)
    second = hidden_of(slots_in, [(gates[j], ups[j]) for j in (far, far ^ near)])
    first_far = swapped(after(first, ups[far]), "tp", far)
    second_far = swapped(second, "tp", far)
    done_own = results_of(place, 0, first, second, down_own, down_near, sizes)
    back_own = exchange(done_own, "ep", direct)

    normed = {0: after(rms_rows(mixer_in, mixer_gain), ups[far], first)}
    normed[far] = swapped(normed[0], "tp", far)
    normed[near] = swapped(normed[0], "tp", near)
    normed = {j: after(normed[j], done_own[0]) for j in normed}
    normed[far ^ near] = swapped(normed[far], "tp", near)
    mixer_rows = jnp.zeros((tp_count * tok_dev, mixer_in.shape[1]), jnp.bfloat16)
    for j in order:
        mixer_rows = lax.dynamic_update_slice_in_dim(
            mixer_rows, normed[j], (tp_index ^ j) * tok_dev, 0
        )
    chan_width = in_gate_weight.shape[1]
    in_gate = jnp.dot(mixer_rows, in_gate_weight, preferred_element_type=jnp.float32)
    values = jnp.dot(mixer_rows, value_weight, preferred_element_type=jnp.float32)
    product = (in_gate * values).astype(jnp.bfloat16)
    out_gate = jnp.dot(mixer_rows, out_gate_weight, preferred_element_type=jnp.float32)
    tap_count = conv_taps.shape[0]
    row_count = product.shape[0]
    rim_rows = lax.ppermute(
        product[row_count - (tap_count - 1) :], "ep", [(i, i + 1) for i in range(ep_count - 1)]
    )
    extended = jnp.concatenate([rim_rows, product], axis=0).astype(jnp.float32)
    tap_rows = lax.dynamic_slice_in_dim(conv_taps, tp_index * chan_width, chan_width, 1)
    conv_sum = tap_rows[0] * extended[0:row_count]
    for tap_index in range(1, tap_count):
        conv_sum = conv_sum + tap_rows[tap_index] * extended[tap_index : tap_index + row_count]
    gated = {0: (out_gate * conv_sum).astype(jnp.bfloat16)}
    gated[far] = swapped(gated[0], "tp", far)
    gated[near] = swapped(gated[0], "tp", near)
    gated[far ^ near] = swapped(gated[far], "tp", near)
    mixer_sum = None
    for j in order:
        term = jnp.dot(
            gated[j], rows_of(mixer_proj, j, chan_width), preferred_element_type=jnp.float32
        )
        mixer_sum = term if mixer_sum is None else mixer_sum + term
    first_far = after(first_far, gated[0])
    done_far = results_of(place, far, first_far, second_far, down_own, down_near, sizes)
    back_far = exchange(done_far, "ep", direct)

    def returned(parts):
        return jnp.concatenate(parts, axis=0)

    shares = route_weights / jnp.sum(route_weights, axis=1, keepdims=True)
    mixed_own = combine_rows(mask_own, hits_own, block_of(shares, 0).T, returned(back_own))
    mixed_far = combine_rows(mask_far, hits_far, block_of(shares, far).T, returned(back_far))
    mixed = jnp.concatenate([mixed_own, mixed_far], axis=0)
    col_width = down_own.shape[1]
    mixed_near = swapped(mixed[:, col_width:], "tp", near)
    expert_out = jnp.zeros((tp_count * tok_dev, col_width), jnp.bfloat16)
    for j, block in (
        (0, mixed[:tok_dev, :col_width]),
        (far, mixed[tok_dev:, :col_width]),
        (near, mixed_near[:tok_dev]),
        (far ^ near, mixed_near[tok_dev:]),
    ):
        expert_out = lax.dynamic_update_slice_in_dim(
            expert_out, block, (tp_index ^ j) * tok_dev, 0
        )

    return (mixer_sum.astype(jnp.bfloat16), expert_out)


def solution(mesh):
    return jax.shard_map(
        on_device,
        mesh=mesh,
        in_specs=(
            P(("ep", "tp"), None),
            P(("ep", "tp"), None),
            P(),
            P(None, "tp"),
            P(None, "tp"),
            P(None, "tp"),
            P(),
            P(None, "tp"),
            P(),
            P("ep", None),
            P("ep", None),
            P("ep", None, "tp"),
            P("ep", None, "tp"),
            P("ep", None, "tp"),
        ),
        out_specs=(P("ep", "tp"), P("ep", "tp")),
        check_vma=False,
    )
```

```python
import functools

import jax
import jax.numpy as jnp
from jax import lax
from jax.experimental import pallas as pl
from jax.experimental.pallas import tpu as pltpu
from jax.sharding import PartitionSpec as P


norm_eps = 1e-06


def rms_rows(values, gain_row):
    wide = values.astype(jnp.float32)
    scale = lax.rsqrt(jnp.mean(wide * wide, axis=-1, keepdims=True) + norm_eps)
    return (wide * scale * gain_row).astype(jnp.bfloat16)


def swapped(value, axis, mask):
    count = lax.axis_size(axis)
    return lax.ppermute(value, axis, [(source, source ^ mask) for source in range(count)])


def after(value, *earlier):
    return lax.optimization_barrier((value, earlier))[0]


def slot_masks(block_ids, labels, slot_cap):
    rows = block_ids.shape[1]
    hits = block_ids[:, None, :] == labels[None, :, None]
    member = jnp.any(hits, axis=0)
    order = jnp.arange(rows, dtype=jnp.int32)
    before = (order[:, None] < order[None, :]).astype(jnp.bfloat16)
    rank = jnp.dot(member.astype(jnp.bfloat16), before, preferred_element_type=jnp.float32)
    rank = jnp.where(member, rank, -1.0)
    slots = jnp.arange(slot_cap, dtype=jnp.int32).astype(jnp.float32)
    return hits, rank[:, None, :] == slots[None, :, None]


def swaps_direct(count):
    return count <= 16 and count & (count - 1) == 0


def far_first(count):
    return sorted(range(1, count), key=lambda k: (-k.bit_length(), k))


def exchange(chunks, axis, direct):
    if direct:
        moved = dict(chunks)
        for k in far_first(lax.axis_size(axis)):
            if k in chunks:
                moved[k] = swapped(chunks[k], axis, k)
        return moved
    rows = chunks[0]
    split = rows.reshape(lax.axis_size(axis), -1, rows.shape[1])
    moved = lax.all_to_all(split, axis, split_axis=0, concat_axis=0, tiled=True)
    return {0: moved.reshape(rows.shape)}


MIB = 1 << 20
STREAMS = 4
ANY = pl.BlockSpec(memory_space=pl.ANY)
VMEM = pl.BlockSpec(memory_space=pltpu.VMEM)
SMEM = pl.BlockSpec(memory_space=pltpu.SMEM)


def dispatch_kernel(direct, slot_cap, place_ref, ids_ref, source_ref, gain_ref, *refs):
    out_refs, (rows_ref, sem) = refs[:-2], refs[-2:]
    load = pltpu.make_async_copy(source_ref, rows_ref, sem)
    load.start()
    tok, width = rows_ref.shape
    total = ids_ref.shape[1]
    slots = sum(ref.shape[0] for ref in out_refs)
    experts = slots // slot_cap
    lanes = min(total, -(-tok // 128) * 128)
    tp_index, ep_index = place_ref[0], place_ref[1]
    ids = pltpu.roll(ids_ref[...], lax.rem(total - tp_index * tok, total), 1)[:, :lanes]
    labels = lax.broadcasted_iota(jnp.int32, (experts, lanes), 0)
    if direct:
        labels = labels ^ ep_index
    member = ids[0:1] == labels
    for pick in range(1, ids_ref.shape[0]):
        member = member | (ids[pick : pick + 1] == labels)
    first = lax.broadcasted_iota(jnp.int32, (lanes, lanes), 0)
    second = lax.broadcasted_iota(jnp.int32, (lanes, lanes), 1)
    before = jnp.where(first < second, 1.0, 0.0).astype(jnp.bfloat16)
    member = jnp.where(member, 1.0, 0.0)
    rank = jnp.dot(member.astype(jnp.bfloat16), before, preferred_element_type=jnp.float32)
    rank = jnp.where(member > 0.5, rank, -1.0).astype(jnp.bfloat16)
    slot = lax.broadcasted_iota(jnp.int32, (slots, experts), 0)
    start = lax.broadcasted_iota(jnp.int32, (slots, experts), 1) * slot_cap
    inside = (slot >= start) & (slot < start + slot_cap)
    spread = jnp.where(inside, 1.0, 0.0)
    rank_of = jnp.dot(spread.astype(jnp.bfloat16), rank, preferred_element_type=jnp.float32)
    offset = jnp.where(inside, (slot - start).astype(jnp.float32), 0.0)
    offset = jnp.sum(offset, axis=1, keepdims=True)
    mask = jnp.where(rank_of == offset, 1.0, 0.0)[:, :tok].astype(jnp.bfloat16)
    load.wait()
    wide = rows_ref[...].astype(jnp.float32)
    scale = lax.rsqrt(jnp.mean(wide * wide, axis=-1, keepdims=True) + norm_eps)
    normed = (wide * scale * gain_ref[...]).astype(jnp.bfloat16)
    step = min(width, 512)
    for col in range(0, width, step):
        part = jnp.dot(mask, normed[:, col : col + step], preferred_element_type=jnp.float32)
        part = part.astype(jnp.bfloat16)
        row = 0
        for ref in out_refs:
            ref[:, col : col + step] = part[row : row + ref.shape[0]]
            row += ref.shape[0]


def dispatched(place, ids, rows, gain, sizes, direct, slot_cap):
    width = rows.shape[1]
    return pl.pallas_call(
        functools.partial(dispatch_kernel, direct, slot_cap),
        out_shape=[jax.ShapeDtypeStruct((size, width), jnp.bfloat16) for size in sizes],
        in_specs=[SMEM, VMEM, ANY, VMEM],
        out_specs=[VMEM] * len(sizes),
        scratch_shapes=[pltpu.VMEM(rows.shape, rows.dtype), pltpu.SemaphoreType.DMA],
        compiler_params=pltpu.CompilerParams(vmem_limit_bytes=56 * MIB),
        cost_estimate=pl.CostEstimate(
            flops=2 * sum(sizes) * rows.shape[0] * width, bytes_accessed=2 * MIB, transcendentals=0
        ),
        name="dispatch",
    )(place, ids, rows, gain)


def stream_hidden(row_refs, weight_refs, rows, weights, row_sems, weight_sems):
    chunks = row_sems.shape[0]
    depth = rows.shape[1] // chunks
    plan = []
    for chunk in range(chunks):
        part = pl.ds(chunk * depth, depth)
        copies, row = [], 0
        for index, ref in enumerate(row_refs):
            target = rows.at[pl.ds(row, ref.shape[0]), part]
            sem = row_sems.at[chunk, index]
            copies.append(pltpu.make_async_copy(ref.at[:, part], target, sem))
            row += ref.shape[0]
        for index, ref in enumerate(weight_refs):
            width = ref.shape[1]
            target = weights.at[index % 2, part, pl.ds(index // 2 * width, width)]
            sem = weight_sems.at[chunk, index]
            copies.append(pltpu.make_async_copy(ref.at[part, :], target, sem))
        for copy in copies:
            copy.start()
        plan.append(copies)
    gate_pre = up_pre = None
    for chunk in range(chunks):
        for copy in plan[chunk]:
            copy.wait()
        part = slice(chunk * depth, (chunk + 1) * depth)
        here = rows[:, part]
        gate_term = jnp.dot(here, weights[0, part, :], preferred_element_type=jnp.float32)
        up_term = jnp.dot(here, weights[1, part, :], preferred_element_type=jnp.float32)
        gate_pre = gate_term if gate_pre is None else gate_pre + gate_term
        up_pre = up_term if up_pre is None else up_pre + up_term
    return (gate_pre / (1.0 + jnp.exp(-gate_pre)) * up_pre).astype(jnp.bfloat16)


def hidden_scratch(row_parts, weights):
    rows = sum(part.shape[0] for part in row_parts)
    depth, width = weights[0].shape
    return [
        pltpu.VMEM((rows, depth), jnp.bfloat16),
        pltpu.VMEM((2, depth, width * len(weights) // 2), jnp.bfloat16),
        pltpu.SemaphoreType.DMA((STREAMS, len(row_parts))),
        pltpu.SemaphoreType.DMA((STREAMS, len(weights))),
    ]


def hidden_cost(row_parts, weights):
    rows = sum(part.shape[0] for part in row_parts)
    depth, width = weights[0].shape
    return pl.CostEstimate(
        flops=2 * rows * depth * width * len(weights),
        bytes_accessed=2 * (rows * depth + len(weights) * depth * width),
        transcendentals=rows * width * len(weights) // 2,
    )


def first_kernel(row_count, *refs):
    row_refs, refs = refs[:row_count], refs[row_count:]
    weight_refs, (out_ref, *scratch) = refs[:-5], refs[-5:]
    out_ref[...] = stream_hidden(row_refs, weight_refs, *scratch)


def first_hidden(row_parts, weights):
    rows = sum(part.shape[0] for part in row_parts)
    width = weights[0].shape[1] * len(weights) // 2
    return pl.pallas_call(
        functools.partial(first_kernel, len(row_parts)),
        out_shape=jax.ShapeDtypeStruct((rows, width), jnp.bfloat16),
        in_specs=[ANY] * (len(row_parts) + len(weights)),
        out_specs=VMEM,
        scratch_shapes=hidden_scratch(row_parts, weights),
        compiler_params=pltpu.CompilerParams(vmem_limit_bytes=56 * MIB),
        cost_estimate=hidden_cost(row_parts, weights),
        name="first_hidden",
    )(*row_parts, *weights)


def down_rows(place, first, second, weight_ref):
    half = first.shape[1] // 2
    total = None
    for j in range(4):
        source = first if j < 2 else second
        block = source[:, (j % 2) * half : (j % 2 + 1) * half]
        start = pl.multiple_of((place ^ j) * half, half)
        term = jnp.dot(block, weight_ref[pl.ds(start, half), :], preferred_element_type=jnp.float32)
        total = term if total is None else total + term
    return total.astype(jnp.bfloat16)


def second_kernel(row_count, weight_count, early_rows, place_ref, first_ref, *refs):
    row_refs, refs = refs[:row_count], refs[row_count:]
    weight_refs, refs = refs[:weight_count], refs[weight_count:]
    down_refs, (hidden_ref, *refs) = refs[:2], refs[2:]
    out_refs, (first_rows, down_own, down_near, down_sems, *scratch) = refs[:-8], refs[-8:]
    sources, targets = (first_ref, *down_refs), (first_rows, down_own, down_near)
    loads = [
        pltpu.make_async_copy(ref, target, down_sems.at[index])
        for index, (ref, target) in enumerate(zip(sources, targets))
    ]
    hidden = stream_hidden(row_refs, weight_refs, *scratch)
    for load in loads:
        load.start()
    hidden_ref[...] = hidden
    loads[0].wait()
    first = first_rows[early_rows:]
    second = hidden_ref[early_rows:]
    col = 0
    for load, weight in zip(loads[1:], (down_own, down_near)):
        load.wait()
        total = down_rows(place_ref[0], first, second, weight)
        row = 0
        for ref in out_refs:
            ref[:, col : col + total.shape[1]] = total[row : row + ref.shape[0]]
            row += ref.shape[0]
        col += total.shape[1]


def second_hidden(place, first, row_parts, weights, downs, sizes, early):
    rows = sum(sizes)
    width = weights[0].shape[1] * len(weights) // 2
    out_width = 2 * downs[0].shape[1]
    outs = [jax.ShapeDtypeStruct((rows, width), jnp.bfloat16)]
    outs += [jax.ShapeDtypeStruct((sizes[k], out_width), jnp.bfloat16) for k in early]
    hidden, *results = pl.pallas_call(
        functools.partial(second_kernel, len(row_parts), len(weights), sum(sizes[: early[0]])),
        out_shape=outs,
        in_specs=[SMEM, ANY] + [ANY] * (len(row_parts) + len(weights) + 2),
        out_specs=[VMEM] * len(outs),
        scratch_shapes=[
            pltpu.VMEM(first.shape, jnp.bfloat16),
            pltpu.VMEM(downs[0].shape, jnp.bfloat16),
            pltpu.VMEM(downs[1].shape, jnp.bfloat16),
            pltpu.SemaphoreType.DMA((3,)),
        ]
        + hidden_scratch(row_parts, weights),
        compiler_params=pltpu.CompilerParams(vmem_limit_bytes=56 * MIB),
        cost_estimate=pl.CostEstimate(flops=MIB, bytes_accessed=MIB, transcendentals=0),
        name="second_hidden",
    )(place, first, *row_parts, *weights, *downs)
    return hidden, dict(zip(early, results))


def late_kernel(far, sizes, early, place_ref, *refs):
    first_ref, second_ref, first_far_ref, second_far_ref, own_ref, near_ref, *refs = refs
    out_refs, (down_own, down_near, sems) = refs[:-3], refs[-3:]
    loads = [
        pltpu.make_async_copy(own_ref, down_own, sems.at[0]),
        pltpu.make_async_copy(near_ref, down_near, sems.at[1]),
    ]
    for load in loads:
        load.start()
    later = [k for k in range(len(sizes)) if k not in early]
    own_rows = sum(sizes[k] for k in later)
    col = 0
    for load, weight_ref in zip(loads, (down_own, down_near)):
        load.wait()
        total = down_rows(place_ref[0] ^ far, first_far_ref[...], second_far_ref[...], weight_ref)
        width = total.shape[1]
        row = 0
        for k, ref in enumerate(out_refs):
            at = 0 if k in early else sizes[k]
            ref[at:, col : col + width] = total[row : row + sizes[k]]
            row += sizes[k]
        if later:
            total = down_rows(place_ref[0], first_ref[:own_rows], second_ref[:own_rows], weight_ref)
            row = 0
            for k in later:
                out_refs[k][: sizes[k], col : col + width] = total[row : row + sizes[k]]
                row += sizes[k]
        col += width


def late_results(place, far, hidden_parts, downs, sizes, early):
    out_width = 2 * downs[0].shape[1]
    rows = [sizes[k] if k in early else 2 * sizes[k] for k in range(len(sizes))]
    return pl.pallas_call(
        functools.partial(late_kernel, far, tuple(sizes), tuple(early)),
        out_shape=[jax.ShapeDtypeStruct((count, out_width), jnp.bfloat16) for count in rows],
        in_specs=[SMEM] + [VMEM] * 4 + [ANY] * 2,
        out_specs=[VMEM] * len(rows),
        scratch_shapes=[
            pltpu.VMEM(downs[0].shape, jnp.bfloat16),
            pltpu.VMEM(downs[1].shape, jnp.bfloat16),
            pltpu.SemaphoreType.DMA((2,)),
        ],
        compiler_params=pltpu.CompilerParams(vmem_limit_bytes=56 * MIB),
        cost_estimate=pl.CostEstimate(
            flops=2 * sum(rows) * downs[0].shape[0] * out_width,
            bytes_accessed=4 * MIB,
            transcendentals=0,
        ),
        name="late_down",
    )(place, *hidden_parts, *downs)


def front_kernel(place_ref, *refs):
    part_refs, weight_refs, refs = refs[:4], refs[4:7], refs[7:]
    product_ref, gate_ref, rows, weights, row_sems, weight_sems = refs
    tok = part_refs[0].shape[0]
    copies = []
    for j, ref in enumerate(part_refs):
        start = pl.multiple_of((place_ref[0] ^ j) * tok, tok)
        copies.append(pltpu.make_async_copy(ref, rows.at[pl.ds(start, tok)], row_sems.at[j]))
    loads = [
        pltpu.make_async_copy(ref, weights.at[index], weight_sems.at[index])
        for index, ref in enumerate(weight_refs)
    ]
    for copy in copies + loads:
        copy.start()
    for copy in copies:
        copy.wait()
    loads[0].wait()
    in_gate = jnp.dot(rows[...], weights[0], preferred_element_type=jnp.float32)
    loads[1].wait()
    values = jnp.dot(rows[...], weights[1], preferred_element_type=jnp.float32)
    product_ref[...] = (in_gate * values).astype(jnp.bfloat16)
    loads[2].wait()
    gate_ref[...] = jnp.dot(rows[...], weights[2], preferred_element_type=jnp.float32)


def mixer_front(place, parts, weights):
    rows = sum(part.shape[0] for part in parts)
    depth, width = weights[0].shape
    return pl.pallas_call(
        front_kernel,
        out_shape=[
            jax.ShapeDtypeStruct((rows, width), jnp.bfloat16),
            jax.ShapeDtypeStruct((rows, width), jnp.float32),
        ],
        in_specs=[SMEM] + [ANY] * 7,
        out_specs=[VMEM, VMEM],
        scratch_shapes=[
            pltpu.VMEM((rows, depth), jnp.bfloat16),
            pltpu.VMEM((3, depth, width), jnp.bfloat16),
            pltpu.SemaphoreType.DMA((4,)),
            pltpu.SemaphoreType.DMA((3,)),
        ],
        compiler_params=pltpu.CompilerParams(vmem_limit_bytes=40 * MIB),
        cost_estimate=pl.CostEstimate(
            flops=6 * rows * depth * width, bytes_accessed=8 * MIB, transcendentals=0
        ),
        name="mixer_front",
    )(place, *parts, *weights)


def share_masks(mask, hits, share_rows):
    share_of = jnp.sum(jnp.where(hits, share_rows[:, None, :], 0.0), axis=0)
    mixed = jnp.where(mask, share_of[:, None, :], 0.0).reshape(-1, mask.shape[2])
    high = mixed.astype(jnp.bfloat16)
    return high, (mixed - high.astype(jnp.float32)).astype(jnp.bfloat16)


def combine_rows(masks, returned):
    dims = (((0,), (0,)), ((), ()))
    total = lax.dot_general(masks[0], returned, dims, preferred_element_type=jnp.float32)
    total = total + lax.dot_general(masks[1], returned, dims, preferred_element_type=jnp.float32)
    return total.astype(jnp.bfloat16)


def on_device(
    mixer_in,
    expert_in,
    mixer_gain,
    in_gate_weight,
    out_gate_weight,
    value_weight,
    conv_taps,
    mixer_proj,
    expert_gain,
    route_ids,
    route_weights,
    gate_weight,
    up_weight,
    down_weight,
):
    tok_dev = mixer_in.shape[0]
    tp_count = lax.axis_size("tp")
    ep_count = lax.axis_size("ep")
    top_count = route_ids.shape[1]
    experts = ep_count * gate_weight.shape[0]
    slot_cap = max(2, 2 * tok_dev * top_count // experts)
    tp_index = lax.axis_index("tp")
    ep_index = lax.axis_index("ep")
    direct = swaps_direct(ep_count)
    near, far = 1, tp_count // 2

    gates, ups = {0: gate_weight[0]}, {0: up_weight[0]}
    gates[far] = swapped(gates[0], "tp", far)
    ups[far] = swapped(ups[0], "tp", far)
    gates[near] = swapped(gates[0], "tp", near)
    ups[near] = swapped(ups[0], "tp", near)
    down_own = down_weight[0]
    down_near = swapped(down_own, "tp", near)
    order = [0, near, far, far ^ near]

    def rows_of(weight, j, width):
        return lax.dynamic_slice_in_dim(weight, (tp_index ^ j) * width, width, 0)

    peers = jnp.arange(experts, dtype=jnp.int32)
    labels = (peers ^ ep_index) if direct else peers

    def block_of(values, j):
        return lax.dynamic_slice_in_dim(values, (tp_index ^ j) * tok_dev, tok_dev, 0)

    hits_own, mask_own = slot_masks(block_of(route_ids, 0).T, labels, slot_cap)
    hits_far, mask_far = slot_masks(block_of(route_ids, far).T, labels, slot_cap)
    shares = route_weights / jnp.sum(route_weights, axis=1, keepdims=True)
    masks_own = share_masks(mask_own, hits_own, block_of(shares, 0).T)
    masks_far = share_masks(mask_far, hits_far, block_of(shares, far).T)
    chan_width = in_gate_weight.shape[1]
    tap_count = conv_taps.shape[0]
    tap_rows = lax.dynamic_slice_in_dim(conv_taps, tp_index * chan_width, chan_width, 1)
    tap_rows = [tap_rows[tap_index] for tap_index in range(tap_count)]
    mixer_normed = rms_rows(mixer_in, mixer_gain)
    place = jnp.where(jnp.arange(2) == 0, tp_index, ep_index).astype(jnp.int32)
    sizes = [slot_cap] * experts if direct else [experts * slot_cap]
    early = list(range(len(sizes) // 2, len(sizes)))
    outgoing = dispatched(
        place, route_ids.T, expert_in, expert_gain[None, :], sizes, direct, slot_cap
    )
    arrived = exchange(dict(enumerate(outgoing)), "ep", direct)
    gates[far ^ near] = swapped(gates[far], "tp", near)
    ready = (masks_own, masks_far, mixer_normed, gates[far ^ near])
    ready += (gates[near], ups[near], down_near)
    arrived[0] = after(arrived[0], *ready)
    slots_in = [arrived[k] for k in range(len(sizes))]

    first = first_hidden(slots_in, [half[j] for j in (0, near) for half in (gates, ups)])
    ups[far ^ near] = swapped(after(ups[far], first), "tp", near)
    downs = (down_own, down_near)
    second, done_own = second_hidden(
        place,
        first,
        slots_in,
        [half[j] for j in (far, far ^ near) for half in (gates, ups)],
        downs,
        sizes,
        early,
    )
    first_far = swapped(after(first, ups[far]), "tp", far)
    second_far = swapped(second, "tp", far)
    back_own = exchange(done_own, "ep", direct)

    normed = {0: after(mixer_normed, ups[far], first)}
    normed[far] = swapped(normed[0], "tp", far)
    normed[near] = swapped(normed[0], "tp", near)
    normed = {j: after(normed[j], second) for j in normed}
    normed[far ^ near] = swapped(normed[far], "tp", near)
    product, out_gate = mixer_front(
        place, [normed[j] for j in order], [in_gate_weight, value_weight, out_gate_weight]
    )
    row_count = product.shape[0]
    rim_rows = lax.ppermute(
        product[row_count - (tap_count - 1) :], "ep", [(i, i + 1) for i in range(ep_count - 1)]
    )
    extended = jnp.concatenate([rim_rows, product], axis=0).astype(jnp.float32)
    conv_sum = tap_rows[0] * extended[0:row_count]
    for tap_index in range(1, tap_count):
        conv_sum = conv_sum + tap_rows[tap_index] * extended[tap_index : tap_index + row_count]
    gated = {0: (out_gate * conv_sum).astype(jnp.bfloat16)}
    gated[far] = swapped(gated[0], "tp", far)
    gated[near] = swapped(gated[0], "tp", near)
    gated[far ^ near] = swapped(gated[far], "tp", near)
    mixer_sum = None
    for j in order:
        term = jnp.dot(
            gated[j], rows_of(mixer_proj, j, chan_width), preferred_element_type=jnp.float32
        )
        mixer_sum = term if mixer_sum is None else mixer_sum + term
    first_far = after(first_far, gated[0])
    late = late_results(place, far, (first, second, first_far, second_far), downs, sizes, early)
    back_late = exchange(dict(enumerate(late)), "ep", direct)
    back_late[0] = after(back_late[0], mixer_sum)
    own_rows = [back_own[k] if k in early else back_late[k][: sizes[k]] for k in range(len(sizes))]
    far_rows = [back_late[k][-sizes[k] :] for k in range(len(sizes))]
    mixed_own = combine_rows(masks_own, jnp.concatenate(own_rows, axis=0))
    mixed_far = combine_rows(masks_far, jnp.concatenate(far_rows, axis=0))
    mixed = jnp.concatenate([mixed_own, mixed_far], axis=0)
    col_width = down_own.shape[1]
    mixed_near = swapped(mixed[:, col_width:], "tp", near)
    expert_out = jnp.zeros((tp_count * tok_dev, col_width), jnp.bfloat16)
    for j, block in (
        (0, mixed[:tok_dev, :col_width]),
        (far, mixed[tok_dev:, :col_width]),
        (near, mixed_near[:tok_dev]),
        (far ^ near, mixed_near[tok_dev:]),
    ):
        expert_out = lax.dynamic_update_slice_in_dim(
            expert_out, block, (tp_index ^ j) * tok_dev, 0
        )

    return (mixer_sum.astype(jnp.bfloat16), expert_out)


def solution(mesh):
    return jax.shard_map(
        on_device,
        mesh=mesh,
        in_specs=(
            P(("ep", "tp"), None),
            P(("ep", "tp"), None),
            P(),
            P(None, "tp"),
            P(None, "tp"),
            P(None, "tp"),
            P(),
            P(None, "tp"),
            P(),
            P("ep", None),
            P("ep", None),
            P("ep", None, "tp"),
            P("ep", None, "tp"),
            P("ep", None, "tp"),
        ),
        out_specs=(P("ep", "tp"), P("ep", "tp")),
        check_vma=False,
    )
```

```python
import functools

import jax
import jax.numpy as jnp
from jax import lax
from jax.experimental import pallas as pl
from jax.experimental.pallas import tpu as pltpu
from jax.sharding import PartitionSpec as P


norm_eps = 1e-06


def rms_rows(values, gain_row):
    wide = values.astype(jnp.float32)
    scale = lax.rsqrt(jnp.mean(wide * wide, axis=-1, keepdims=True) + norm_eps)
    return (wide * scale * gain_row).astype(jnp.bfloat16)


def swapped(value, axis, mask):
    count = lax.axis_size(axis)
    return lax.ppermute(value, axis, [(source, source ^ mask) for source in range(count)])


def after(value, *earlier):
    return lax.optimization_barrier((value, earlier))[0]


def slot_masks(block_ids, labels, slot_cap):
    rows = block_ids.shape[1]
    hits = block_ids[:, None, :] == labels[None, :, None]
    member = jnp.any(hits, axis=0)
    order = jnp.arange(rows, dtype=jnp.int32)
    before = (order[:, None] < order[None, :]).astype(jnp.bfloat16)
    rank = jnp.dot(member.astype(jnp.bfloat16), before, preferred_element_type=jnp.float32)
    rank = jnp.where(member, rank, -1.0)
    slots = jnp.arange(slot_cap, dtype=jnp.int32).astype(jnp.float32)
    return hits, rank[:, None, :] == slots[None, :, None]


def swaps_direct(count):
    return count <= 16 and count & (count - 1) == 0


def start_order(count):
    across = [k for k in range(1, count) if k & (count // 2)]
    nearer = [k for k in range(2, count // 2)]
    half = len(across) // 2
    return across[:half] + nearer + across[half:] + [1] * (count > 2)


def exchange(chunks, axis, direct):
    if direct:
        moved = dict(chunks)
        for k in start_order(lax.axis_size(axis)):
            if k in chunks:
                moved[k] = swapped(chunks[k], axis, k)
        return moved
    rows = chunks[0]
    split = rows.reshape(lax.axis_size(axis), -1, rows.shape[1])
    moved = lax.all_to_all(split, axis, split_axis=0, concat_axis=0, tiled=True)
    return {0: moved.reshape(rows.shape)}


MIB = 1 << 20
STREAMS = 4
ANY = pl.BlockSpec(memory_space=pl.ANY)
VMEM = pl.BlockSpec(memory_space=pltpu.VMEM)
SMEM = pl.BlockSpec(memory_space=pltpu.SMEM)


def dispatch_kernel(direct, slot_cap, place_ref, ids_ref, source_ref, gain_ref, *refs):
    out_refs, (rows_ref, sem) = refs[:-2], refs[-2:]
    load = pltpu.make_async_copy(source_ref, rows_ref, sem)
    load.start()
    tok, width = rows_ref.shape
    total = ids_ref.shape[1]
    slots = sum(ref.shape[0] for ref in out_refs)
    experts = slots // slot_cap
    lanes = min(total, -(-tok // 128) * 128)
    tp_index, ep_index = place_ref[0], place_ref[1]
    ids = pltpu.roll(ids_ref[...], lax.rem(total - tp_index * tok, total), 1)[:, :lanes]
    labels = lax.broadcasted_iota(jnp.int32, (experts, lanes), 0)
    if direct:
        labels = labels ^ ep_index
    member = ids[0:1] == labels
    for pick in range(1, ids_ref.shape[0]):
        member = member | (ids[pick : pick + 1] == labels)
    first = lax.broadcasted_iota(jnp.int32, (lanes, lanes), 0)
    second = lax.broadcasted_iota(jnp.int32, (lanes, lanes), 1)
    before = jnp.where(first < second, 1.0, 0.0).astype(jnp.bfloat16)
    member = jnp.where(member, 1.0, 0.0)
    rank = jnp.dot(member.astype(jnp.bfloat16), before, preferred_element_type=jnp.float32)
    rank = jnp.where(member > 0.5, rank, -1.0).astype(jnp.bfloat16)
    slot = lax.broadcasted_iota(jnp.int32, (slots, experts), 0)
    start = lax.broadcasted_iota(jnp.int32, (slots, experts), 1) * slot_cap
    inside = (slot >= start) & (slot < start + slot_cap)
    spread = jnp.where(inside, 1.0, 0.0)
    rank_of = jnp.dot(spread.astype(jnp.bfloat16), rank, preferred_element_type=jnp.float32)
    offset = jnp.where(inside, (slot - start).astype(jnp.float32), 0.0)
    offset = jnp.sum(offset, axis=1, keepdims=True)
    mask = jnp.where(rank_of == offset, 1.0, 0.0)[:, :tok].astype(jnp.bfloat16)
    load.wait()
    wide = rows_ref[...].astype(jnp.float32)
    scale = lax.rsqrt(jnp.mean(wide * wide, axis=-1, keepdims=True) + norm_eps)
    normed = (wide * scale * gain_ref[...]).astype(jnp.bfloat16)
    step = min(width, 512)
    for col in range(0, width, step):
        part = jnp.dot(mask, normed[:, col : col + step], preferred_element_type=jnp.float32)
        part = part.astype(jnp.bfloat16)
        row = 0
        for ref in out_refs:
            ref[:, col : col + step] = part[row : row + ref.shape[0]]
            row += ref.shape[0]


def dispatched(place, ids, rows, gain, sizes, direct, slot_cap):
    width = rows.shape[1]
    return pl.pallas_call(
        functools.partial(dispatch_kernel, direct, slot_cap),
        out_shape=[jax.ShapeDtypeStruct((size, width), jnp.bfloat16) for size in sizes],
        in_specs=[SMEM, VMEM, ANY, VMEM],
        out_specs=[VMEM] * len(sizes),
        scratch_shapes=[pltpu.VMEM(rows.shape, rows.dtype), pltpu.SemaphoreType.DMA],
        compiler_params=pltpu.CompilerParams(vmem_limit_bytes=56 * MIB),
        cost_estimate=pl.CostEstimate(
            flops=2 * sum(sizes) * rows.shape[0] * width, bytes_accessed=2 * MIB, transcendentals=0
        ),
        name="dispatch",
    )(place, ids, rows, gain)


def stream_hidden(row_refs, weight_refs, rows, weights, row_sems, weight_sems, later=()):
    chunks = row_sems.shape[0]
    depth = rows.shape[1] // chunks
    plan = []
    for chunk in range(chunks):
        part = pl.ds(chunk * depth, depth)
        copies, row = [], 0
        for index, ref in enumerate(row_refs):
            target = rows.at[pl.ds(row, ref.shape[0]), part]
            sem = row_sems.at[chunk, index]
            copies.append(pltpu.make_async_copy(ref.at[:, part], target, sem))
            row += ref.shape[0]
        for index, ref in enumerate(weight_refs):
            width = ref.shape[1]
            target = weights.at[index % 2, part, pl.ds(index // 2 * width, width)]
            sem = weight_sems.at[chunk, index]
            copies.append(pltpu.make_async_copy(ref.at[part, :], target, sem))
        for copy in copies:
            copy.start()
        plan.append(copies)
    gate_pre = up_pre = None
    for chunk in range(chunks):
        for copy in plan[chunk]:
            copy.wait()
        if chunk == 0:
            for copy in later:
                copy.start()
        part = slice(chunk * depth, (chunk + 1) * depth)
        here = rows[:, part]
        gate_term = jnp.dot(here, weights[0, part, :], preferred_element_type=jnp.float32)
        up_term = jnp.dot(here, weights[1, part, :], preferred_element_type=jnp.float32)
        gate_pre = gate_term if gate_pre is None else gate_pre + gate_term
        up_pre = up_term if up_pre is None else up_pre + up_term
    return (gate_pre / (1.0 + jnp.exp(-gate_pre)) * up_pre).astype(jnp.bfloat16)


def hidden_scratch(row_parts, weights):
    rows = sum(part.shape[0] for part in row_parts)
    depth, width = weights[0].shape
    return [
        pltpu.VMEM((rows, depth), jnp.bfloat16),
        pltpu.VMEM((2, depth, width * len(weights) // 2), jnp.bfloat16),
        pltpu.SemaphoreType.DMA((STREAMS, len(row_parts))),
        pltpu.SemaphoreType.DMA((STREAMS, len(weights))),
    ]


def hidden_cost(row_parts, weights):
    rows = sum(part.shape[0] for part in row_parts)
    depth, width = weights[0].shape
    return pl.CostEstimate(
        flops=2 * rows * depth * width * len(weights),
        bytes_accessed=2 * (rows * depth + len(weights) * depth * width),
        transcendentals=rows * width * len(weights) // 2,
    )


def first_kernel(row_count, *refs):
    row_refs, refs = refs[:row_count], refs[row_count:]
    weight_refs, (out_ref, *scratch) = refs[:-5], refs[-5:]
    out_ref[...] = stream_hidden(row_refs, weight_refs, *scratch)


def first_hidden(row_parts, weights):
    rows = sum(part.shape[0] for part in row_parts)
    width = weights[0].shape[1] * len(weights) // 2
    return pl.pallas_call(
        functools.partial(first_kernel, len(row_parts)),
        out_shape=jax.ShapeDtypeStruct((rows, width), jnp.bfloat16),
        in_specs=[ANY] * (len(row_parts) + len(weights)),
        out_specs=VMEM,
        scratch_shapes=hidden_scratch(row_parts, weights),
        compiler_params=pltpu.CompilerParams(vmem_limit_bytes=56 * MIB),
        cost_estimate=hidden_cost(row_parts, weights),
        name="first_hidden",
    )(*row_parts, *weights)


def down_rows(place, first, second, weight_ref):
    half = first.shape[1] // 2
    total = None
    for j in range(4):
        source = first if j < 2 else second
        block = source[:, (j % 2) * half : (j % 2 + 1) * half]
        start = pl.multiple_of((place ^ j) * half, half)
        term = jnp.dot(block, weight_ref[pl.ds(start, half), :], preferred_element_type=jnp.float32)
        total = term if total is None else total + term
    return total.astype(jnp.bfloat16)


def second_kernel(row_count, weight_count, early_rows, place_ref, first_ref, *refs):
    row_refs, refs = refs[:row_count], refs[row_count:]
    weight_refs, refs = refs[:weight_count], refs[weight_count:]
    down_refs, (hidden_ref, *refs) = refs[:2], refs[2:]
    out_refs, (first_rows, down_own, down_near, down_sems, *scratch) = refs[:-8], refs[-8:]
    sources, targets = (first_ref, *down_refs), (first_rows, down_own, down_near)
    loads = [
        pltpu.make_async_copy(ref, target, down_sems.at[index])
        for index, (ref, target) in enumerate(zip(sources, targets))
    ]
    hidden_ref[...] = stream_hidden(row_refs, weight_refs, *scratch, later=loads)
    loads[0].wait()
    first = first_rows[early_rows:]
    second = hidden_ref[early_rows:]
    col = 0
    for load, weight in zip(loads[1:], (down_own, down_near)):
        load.wait()
        total = down_rows(place_ref[0], first, second, weight)
        row = 0
        for ref in out_refs:
            ref[:, col : col + total.shape[1]] = total[row : row + ref.shape[0]]
            row += ref.shape[0]
        col += total.shape[1]


def second_hidden(place, first, row_parts, weights, downs, sizes, early):
    rows = sum(sizes)
    width = weights[0].shape[1] * len(weights) // 2
    out_width = 2 * downs[0].shape[1]
    outs = [jax.ShapeDtypeStruct((rows, width), jnp.bfloat16)]
    outs += [jax.ShapeDtypeStruct((sizes[k], out_width), jnp.bfloat16) for k in early]
    hidden, *results = pl.pallas_call(
        functools.partial(second_kernel, len(row_parts), len(weights), sum(sizes[: early[0]])),
        out_shape=outs,
        in_specs=[SMEM, ANY] + [ANY] * (len(row_parts) + len(weights) + 2),
        out_specs=[VMEM] * len(outs),
        scratch_shapes=[
            pltpu.VMEM(first.shape, jnp.bfloat16),
            pltpu.VMEM(downs[0].shape, jnp.bfloat16),
            pltpu.VMEM(downs[1].shape, jnp.bfloat16),
            pltpu.SemaphoreType.DMA((3,)),
        ]
        + hidden_scratch(row_parts, weights),
        compiler_params=pltpu.CompilerParams(vmem_limit_bytes=56 * MIB),
        cost_estimate=pl.CostEstimate(flops=MIB, bytes_accessed=MIB, transcendentals=0),
        name="second_hidden",
    )(place, first, *row_parts, *weights, *downs)
    return hidden, dict(zip(early, results))


def late_kernel(far, sizes, early, place_ref, *refs):
    first_ref, second_ref, first_far_ref, second_far_ref, own_ref, near_ref, *refs = refs
    out_refs, (down_own, down_near, sems) = refs[:-3], refs[-3:]
    loads = [
        pltpu.make_async_copy(own_ref, down_own, sems.at[0]),
        pltpu.make_async_copy(near_ref, down_near, sems.at[1]),
    ]
    for load in loads:
        load.start()
    later = [k for k in range(len(sizes)) if k not in early]
    own_rows = sum(sizes[k] for k in later)
    col = 0
    for load, weight_ref in zip(loads, (down_own, down_near)):
        load.wait()
        total = down_rows(place_ref[0] ^ far, first_far_ref[...], second_far_ref[...], weight_ref)
        width = total.shape[1]
        row = 0
        for k, ref in enumerate(out_refs):
            at = 0 if k in early else sizes[k]
            ref[at:, col : col + width] = total[row : row + sizes[k]]
            row += sizes[k]
        if later:
            total = down_rows(place_ref[0], first_ref[:own_rows], second_ref[:own_rows], weight_ref)
            row = 0
            for k in later:
                out_refs[k][: sizes[k], col : col + width] = total[row : row + sizes[k]]
                row += sizes[k]
        col += width


def late_results(place, far, hidden_parts, downs, sizes, early):
    out_width = 2 * downs[0].shape[1]
    rows = [sizes[k] if k in early else 2 * sizes[k] for k in range(len(sizes))]
    return pl.pallas_call(
        functools.partial(late_kernel, far, tuple(sizes), tuple(early)),
        out_shape=[jax.ShapeDtypeStruct((count, out_width), jnp.bfloat16) for count in rows],
        in_specs=[SMEM] + [VMEM] * 4 + [ANY] * 2,
        out_specs=[VMEM] * len(rows),
        scratch_shapes=[
            pltpu.VMEM(downs[0].shape, jnp.bfloat16),
            pltpu.VMEM(downs[1].shape, jnp.bfloat16),
            pltpu.SemaphoreType.DMA((2,)),
        ],
        compiler_params=pltpu.CompilerParams(vmem_limit_bytes=24 * MIB),
        cost_estimate=pl.CostEstimate(
            flops=2 * sum(rows) * downs[0].shape[0] * out_width,
            bytes_accessed=4 * MIB,
            transcendentals=0,
        ),
        name="late_down",
    )(place, *hidden_parts, *downs)


def front_kernel(place_ref, *refs):
    part_refs, weight_refs, refs = refs[:4], refs[4:7], refs[7:]
    product_ref, gate_ref, rows, weights, row_sems, weight_sems = refs
    tok = part_refs[0].shape[0]
    copies = []
    for j, ref in enumerate(part_refs):
        start = pl.multiple_of((place_ref[0] ^ j) * tok, tok)
        copies.append(pltpu.make_async_copy(ref, rows.at[pl.ds(start, tok)], row_sems.at[j]))
    loads = [
        pltpu.make_async_copy(ref, weights.at[index], weight_sems.at[index])
        for index, ref in enumerate(weight_refs)
    ]
    for copy in copies + loads:
        copy.start()
    for copy in copies:
        copy.wait()
    loads[0].wait()
    in_gate = jnp.dot(rows[...], weights[0], preferred_element_type=jnp.float32)
    loads[1].wait()
    values = jnp.dot(rows[...], weights[1], preferred_element_type=jnp.float32)
    product_ref[...] = (in_gate * values).astype(jnp.bfloat16)
    loads[2].wait()
    gate_ref[...] = jnp.dot(rows[...], weights[2], preferred_element_type=jnp.float32)


def mixer_front(place, parts, weights):
    rows = sum(part.shape[0] for part in parts)
    depth, width = weights[0].shape
    return pl.pallas_call(
        front_kernel,
        out_shape=[
            jax.ShapeDtypeStruct((rows, width), jnp.bfloat16),
            jax.ShapeDtypeStruct((rows, width), jnp.float32),
        ],
        in_specs=[SMEM] + [ANY] * 7,
        out_specs=[VMEM, VMEM],
        scratch_shapes=[
            pltpu.VMEM((rows, depth), jnp.bfloat16),
            pltpu.VMEM((3, depth, width), jnp.bfloat16),
            pltpu.SemaphoreType.DMA((4,)),
            pltpu.SemaphoreType.DMA((3,)),
        ],
        compiler_params=pltpu.CompilerParams(vmem_limit_bytes=56 * MIB),
        cost_estimate=pl.CostEstimate(
            flops=6 * rows * depth * width, bytes_accessed=8 * MIB, transcendentals=0
        ),
        name="mixer_front",
    )(place, *parts, *weights)


def share_masks(mask, hits, share_rows):
    share_of = jnp.sum(jnp.where(hits, share_rows[:, None, :], 0.0), axis=0)
    mixed = jnp.where(mask, share_of[:, None, :], 0.0).reshape(-1, mask.shape[2])
    high = mixed.astype(jnp.bfloat16)
    return high, (mixed - high.astype(jnp.float32)).astype(jnp.bfloat16)


def combine_rows(masks, returned):
    dims = (((0,), (0,)), ((), ()))
    total = lax.dot_general(masks[0], returned, dims, preferred_element_type=jnp.float32)
    total = total + lax.dot_general(masks[1], returned, dims, preferred_element_type=jnp.float32)
    return total.astype(jnp.bfloat16)


def on_device(
    mixer_in,
    expert_in,
    mixer_gain,
    in_gate_weight,
    out_gate_weight,
    value_weight,
    conv_taps,
    mixer_proj,
    expert_gain,
    route_ids,
    route_weights,
    gate_weight,
    up_weight,
    down_weight,
):
    tok_dev = mixer_in.shape[0]
    tp_count = lax.axis_size("tp")
    ep_count = lax.axis_size("ep")
    top_count = route_ids.shape[1]
    experts = ep_count * gate_weight.shape[0]
    slot_cap = max(2, 2 * tok_dev * top_count // experts)
    tp_index = lax.axis_index("tp")
    ep_index = lax.axis_index("ep")
    direct = swaps_direct(ep_count)
    near, far = 1, tp_count // 2

    gates, ups = {0: gate_weight[0]}, {0: up_weight[0]}
    gates[far] = swapped(gates[0], "tp", far)
    ups[far] = swapped(ups[0], "tp", far)
    gates[near] = swapped(gates[0], "tp", near)
    ups[near] = swapped(ups[0], "tp", near)
    down_own = down_weight[0]
    down_near = swapped(down_own, "tp", near)
    order = [0, near, far, far ^ near]

    def rows_of(weight, j, width):
        return lax.dynamic_slice_in_dim(weight, (tp_index ^ j) * width, width, 0)

    peers = jnp.arange(experts, dtype=jnp.int32)
    labels = (peers ^ ep_index) if direct else peers

    def block_of(values, j):
        return lax.dynamic_slice_in_dim(values, (tp_index ^ j) * tok_dev, tok_dev, 0)

    hits_own, mask_own = slot_masks(block_of(route_ids, 0).T, labels, slot_cap)
    hits_far, mask_far = slot_masks(block_of(route_ids, far).T, labels, slot_cap)
    shares = route_weights / jnp.sum(route_weights, axis=1, keepdims=True)
    masks_own = share_masks(mask_own, hits_own, block_of(shares, 0).T)
    masks_far = share_masks(mask_far, hits_far, block_of(shares, far).T)
    chan_width = in_gate_weight.shape[1]
    tap_count = conv_taps.shape[0]
    tap_rows = lax.dynamic_slice_in_dim(conv_taps, tp_index * chan_width, chan_width, 1)
    tap_rows = [tap_rows[tap_index] for tap_index in range(tap_count)]
    mixer_normed = rms_rows(mixer_in, mixer_gain)
    place = jnp.where(jnp.arange(2) == 0, tp_index, ep_index).astype(jnp.int32)
    sizes = [slot_cap] * experts if direct else [experts * slot_cap]
    early = list(range(len(sizes) // 2, len(sizes)))
    outgoing = dispatched(
        place, route_ids.T, expert_in, expert_gain[None, :], sizes, direct, slot_cap
    )
    arrived = exchange(dict(enumerate(outgoing)), "ep", direct)
    gates[far ^ near] = swapped(gates[far], "tp", near)
    ready = (masks_own, masks_far, mixer_normed, gates[far ^ near])
    ready += (gates[near], ups[near], down_near)
    arrived[0] = after(arrived[0], *ready)
    slots_in = [arrived[k] for k in range(len(sizes))]

    first = first_hidden(slots_in, [half[j] for j in (0, near) for half in (gates, ups)])
    ups[far ^ near] = swapped(after(ups[far], first), "tp", near)
    downs = (down_own, down_near)
    second, done_own = second_hidden(
        place,
        first,
        slots_in,
        [half[j] for j in (far, far ^ near) for half in (gates, ups)],
        downs,
        sizes,
        early,
    )
    first_far = swapped(after(first, ups[far]), "tp", far)
    second_far = swapped(second, "tp", far)
    back_own = exchange(done_own, "ep", direct)

    normed = {0: after(mixer_normed, ups[far], first)}
    normed[far] = swapped(normed[0], "tp", far)
    normed[near] = swapped(normed[0], "tp", near)
    normed = {j: after(normed[j], second) for j in normed}
    normed[far ^ near] = swapped(normed[far], "tp", near)
    product, out_gate = mixer_front(
        place, [normed[j] for j in order], [in_gate_weight, value_weight, out_gate_weight]
    )
    row_count = product.shape[0]
    rim_rows = lax.ppermute(
        product[row_count - (tap_count - 1) :], "ep", [(i, i + 1) for i in range(ep_count - 1)]
    )
    extended = jnp.concatenate([rim_rows, product], axis=0).astype(jnp.float32)
    conv_sum = tap_rows[0] * extended[0:row_count]
    for tap_index in range(1, tap_count):
        conv_sum = conv_sum + tap_rows[tap_index] * extended[tap_index : tap_index + row_count]
    gated = {0: (out_gate * conv_sum).astype(jnp.bfloat16)}
    gated[far] = swapped(gated[0], "tp", far)
    gated[near] = swapped(gated[0], "tp", near)
    gated[far ^ near] = swapped(gated[far], "tp", near)
    mixer_sum = None
    for j in order:
        term = jnp.dot(
            gated[j], rows_of(mixer_proj, j, chan_width), preferred_element_type=jnp.float32
        )
        mixer_sum = term if mixer_sum is None else mixer_sum + term
    first_far = after(first_far, product)
    late = late_results(place, far, (first, second, first_far, second_far), downs, sizes, early)
    back_late = exchange(dict(enumerate(late)), "ep", direct)
    back_late[0] = after(back_late[0], mixer_sum)
    own_rows = [back_own[k] if k in early else back_late[k][: sizes[k]] for k in range(len(sizes))]
    far_rows = [back_late[k][-sizes[k] :] for k in range(len(sizes))]
    mixed_own = combine_rows(masks_own, jnp.concatenate(own_rows, axis=0))
    mixed_far = combine_rows(masks_far, jnp.concatenate(far_rows, axis=0))
    mixed = jnp.concatenate([mixed_own, mixed_far], axis=0)
    col_width = down_own.shape[1]
    mixed_near = swapped(mixed[:, col_width:], "tp", near)
    expert_out = jnp.zeros((tp_count * tok_dev, col_width), jnp.bfloat16)
    for j, block in (
        (0, mixed[:tok_dev, :col_width]),
        (far, mixed[tok_dev:, :col_width]),
        (near, mixed_near[:tok_dev]),
        (far ^ near, mixed_near[tok_dev:]),
    ):
        expert_out = lax.dynamic_update_slice_in_dim(
            expert_out, block, (tp_index ^ j) * tok_dev, 0
        )

    return (mixer_sum.astype(jnp.bfloat16), expert_out)


def solution(mesh):
    return jax.shard_map(
        on_device,
        mesh=mesh,
        in_specs=(
            P(("ep", "tp"), None),
            P(("ep", "tp"), None),
            P(),
            P(None, "tp"),
            P(None, "tp"),
            P(None, "tp"),
            P(),
            P(None, "tp"),
            P(),
            P("ep", None),
            P("ep", None),
            P("ep", None, "tp"),
            P("ep", None, "tp"),
            P("ep", None, "tp"),
        ),
        out_specs=(P("ep", "tp"), P("ep", "tp")),
        check_vma=False,
    )
```

```python
import functools

import jax
import jax.numpy as jnp
from jax import lax
from jax.experimental import pallas as pl
from jax.experimental.pallas import tpu as pltpu
from jax.sharding import PartitionSpec as P


norm_eps = 1e-06


def rms_rows(values, gain_row):
    wide = values.astype(jnp.float32)
    scale = lax.rsqrt(jnp.mean(wide * wide, axis=-1, keepdims=True) + norm_eps)
    return (wide * scale * gain_row).astype(jnp.bfloat16)


def swapped(value, axis, mask):
    count = lax.axis_size(axis)
    return lax.ppermute(value, axis, [(source, source ^ mask) for source in range(count)])


def after(value, *earlier):
    return lax.optimization_barrier((value, earlier))[0]


def slot_masks(block_ids, labels, slot_cap):
    rows = block_ids.shape[1]
    hits = block_ids[:, None, :] == labels[None, :, None]
    member = jnp.any(hits, axis=0)
    order = jnp.arange(rows, dtype=jnp.int32)
    before = (order[:, None] < order[None, :]).astype(jnp.bfloat16)
    rank = jnp.dot(member.astype(jnp.bfloat16), before, preferred_element_type=jnp.float32)
    rank = jnp.where(member, rank, -1.0)
    slots = jnp.arange(slot_cap, dtype=jnp.int32).astype(jnp.float32)
    return hits, rank[:, None, :] == slots[None, :, None]


def swaps_direct(count):
    return count <= 16 and count & (count - 1) == 0


def start_order(count):
    across = [k for k in range(1, count) if k & (count // 2)]
    nearer = [k for k in range(2, count // 2)]
    half = len(across) // 2
    return across[:half] + [1] * (count > 2) + nearer + across[half:]


def exchange(chunks, axis, direct):
    if direct:
        moved = dict(chunks)
        for k in start_order(lax.axis_size(axis)):
            if k in chunks:
                moved[k] = swapped(chunks[k], axis, k)
        return moved
    rows = chunks[0]
    split = rows.reshape(lax.axis_size(axis), -1, rows.shape[1])
    moved = lax.all_to_all(split, axis, split_axis=0, concat_axis=0, tiled=True)
    return {0: moved.reshape(rows.shape)}


MIB = 1 << 20
STREAMS = 4
ANY = pl.BlockSpec(memory_space=pl.ANY)
VMEM = pl.BlockSpec(memory_space=pltpu.VMEM)
SMEM = pl.BlockSpec(memory_space=pltpu.SMEM)


def dispatch_kernel(direct, slot_cap, place_ref, ids_ref, source_ref, gain_ref, *refs):
    out_refs, (rows_ref, sem) = refs[:-2], refs[-2:]
    load = pltpu.make_async_copy(source_ref, rows_ref, sem)
    load.start()
    tok, width = rows_ref.shape
    total = ids_ref.shape[1]
    slots = sum(ref.shape[0] for ref in out_refs)
    experts = slots // slot_cap
    lanes = min(total, -(-tok // 128) * 128)
    tp_index, ep_index = place_ref[0], place_ref[1]
    ids = pltpu.roll(ids_ref[...], lax.rem(total - tp_index * tok, total), 1)[:, :lanes]
    labels = lax.broadcasted_iota(jnp.int32, (experts, lanes), 0)
    if direct:
        labels = labels ^ ep_index
    member = ids[0:1] == labels
    for pick in range(1, ids_ref.shape[0]):
        member = member | (ids[pick : pick + 1] == labels)
    first = lax.broadcasted_iota(jnp.int32, (lanes, lanes), 0)
    second = lax.broadcasted_iota(jnp.int32, (lanes, lanes), 1)
    before = jnp.where(first < second, 1.0, 0.0).astype(jnp.bfloat16)
    member = jnp.where(member, 1.0, 0.0)
    rank = jnp.dot(member.astype(jnp.bfloat16), before, preferred_element_type=jnp.float32)
    rank = jnp.where(member > 0.5, rank, -1.0).astype(jnp.bfloat16)
    slot = lax.broadcasted_iota(jnp.int32, (slots, experts), 0)
    start = lax.broadcasted_iota(jnp.int32, (slots, experts), 1) * slot_cap
    inside = (slot >= start) & (slot < start + slot_cap)
    spread = jnp.where(inside, 1.0, 0.0)
    rank_of = jnp.dot(spread.astype(jnp.bfloat16), rank, preferred_element_type=jnp.float32)
    offset = jnp.where(inside, (slot - start).astype(jnp.float32), 0.0)
    offset = jnp.sum(offset, axis=1, keepdims=True)
    mask = jnp.where(rank_of == offset, 1.0, 0.0)[:, :tok].astype(jnp.bfloat16)
    load.wait()
    wide = rows_ref[...].astype(jnp.float32)
    scale = lax.rsqrt(jnp.mean(wide * wide, axis=-1, keepdims=True) + norm_eps)
    normed = (wide * scale * gain_ref[...]).astype(jnp.bfloat16)
    step = min(width, 512)
    for col in range(0, width, step):
        part = jnp.dot(mask, normed[:, col : col + step], preferred_element_type=jnp.float32)
        part = part.astype(jnp.bfloat16)
        row = 0
        for ref in out_refs:
            ref[:, col : col + step] = part[row : row + ref.shape[0]]
            row += ref.shape[0]


def dispatched(place, ids, rows, gain, sizes, direct, slot_cap):
    width = rows.shape[1]
    return pl.pallas_call(
        functools.partial(dispatch_kernel, direct, slot_cap),
        out_shape=[jax.ShapeDtypeStruct((size, width), jnp.bfloat16) for size in sizes],
        in_specs=[SMEM, VMEM, ANY, VMEM],
        out_specs=[VMEM] * len(sizes),
        scratch_shapes=[pltpu.VMEM(rows.shape, rows.dtype), pltpu.SemaphoreType.DMA],
        compiler_params=pltpu.CompilerParams(vmem_limit_bytes=56 * MIB),
        cost_estimate=pl.CostEstimate(
            flops=2 * sum(sizes) * rows.shape[0] * width, bytes_accessed=2 * MIB, transcendentals=0
        ),
        name="dispatch",
    )(place, ids, rows, gain)


def stream_hidden(row_refs, weight_refs, rows, weights, row_sems, weight_sems, later=()):
    chunks = row_sems.shape[0]
    depth = rows.shape[1] // chunks
    plan = []
    for chunk in range(chunks):
        part = pl.ds(chunk * depth, depth)
        copies, row = [], 0
        for index, ref in enumerate(row_refs):
            target = rows.at[pl.ds(row, ref.shape[0]), part]
            sem = row_sems.at[chunk, index]
            copies.append(pltpu.make_async_copy(ref.at[:, part], target, sem))
            row += ref.shape[0]
        for index, ref in enumerate(weight_refs):
            width = ref.shape[1]
            target = weights.at[index % 2, part, pl.ds(index // 2 * width, width)]
            sem = weight_sems.at[chunk, index]
            copies.append(pltpu.make_async_copy(ref.at[part, :], target, sem))
        for copy in copies:
            copy.start()
        plan.append(copies)
    gate_pre = up_pre = None
    for chunk in range(chunks):
        for copy in plan[chunk]:
            copy.wait()
        if chunk == 0:
            for copy in later:
                copy.start()
        part = slice(chunk * depth, (chunk + 1) * depth)
        here = rows[:, part]
        gate_term = jnp.dot(here, weights[0, part, :], preferred_element_type=jnp.float32)
        up_term = jnp.dot(here, weights[1, part, :], preferred_element_type=jnp.float32)
        gate_pre = gate_term if gate_pre is None else gate_pre + gate_term
        up_pre = up_term if up_pre is None else up_pre + up_term
    return (gate_pre / (1.0 + jnp.exp(-gate_pre)) * up_pre).astype(jnp.bfloat16)


def hidden_scratch(row_parts, weights):
    rows = sum(part.shape[0] for part in row_parts)
    depth, width = weights[0].shape
    return [
        pltpu.VMEM((rows, depth), jnp.bfloat16),
        pltpu.VMEM((2, depth, width * len(weights) // 2), jnp.bfloat16),
        pltpu.SemaphoreType.DMA((STREAMS, len(row_parts))),
        pltpu.SemaphoreType.DMA((STREAMS, len(weights))),
    ]


def hidden_cost(row_parts, weights):
    rows = sum(part.shape[0] for part in row_parts)
    depth, width = weights[0].shape
    return pl.CostEstimate(
        flops=2 * rows * depth * width * len(weights),
        bytes_accessed=2 * (rows * depth + len(weights) * depth * width),
        transcendentals=rows * width * len(weights) // 2,
    )


def first_kernel(row_count, *refs):
    row_refs, refs = refs[:row_count], refs[row_count:]
    weight_refs, (out_ref, *scratch) = refs[:-5], refs[-5:]
    out_ref[...] = stream_hidden(row_refs, weight_refs, *scratch)


def first_hidden(row_parts, weights):
    rows = sum(part.shape[0] for part in row_parts)
    width = weights[0].shape[1] * len(weights) // 2
    return pl.pallas_call(
        functools.partial(first_kernel, len(row_parts)),
        out_shape=jax.ShapeDtypeStruct((rows, width), jnp.bfloat16),
        in_specs=[ANY] * (len(row_parts) + len(weights)),
        out_specs=VMEM,
        scratch_shapes=hidden_scratch(row_parts, weights),
        compiler_params=pltpu.CompilerParams(vmem_limit_bytes=56 * MIB),
        cost_estimate=hidden_cost(row_parts, weights),
        name="first_hidden",
    )(*row_parts, *weights)


def down_rows(place, first, second, weight_ref):
    half = first.shape[1] // 2
    total = None
    for j in range(4):
        source = first if j < 2 else second
        block = source[:, (j % 2) * half : (j % 2 + 1) * half]
        start = pl.multiple_of((place ^ j) * half, half)
        term = jnp.dot(block, weight_ref[pl.ds(start, half), :], preferred_element_type=jnp.float32)
        total = term if total is None else total + term
    return total.astype(jnp.bfloat16)


def second_kernel(row_count, weight_count, early_rows, place_ref, first_ref, *refs):
    row_refs, refs = refs[:row_count], refs[row_count:]
    weight_refs, refs = refs[:weight_count], refs[weight_count:]
    down_refs, (hidden_ref, *refs) = refs[:2], refs[2:]
    out_refs, (first_rows, down_own, down_near, down_sems, *scratch) = refs[:-8], refs[-8:]
    sources, targets = (first_ref, *down_refs), (first_rows, down_own, down_near)
    loads = [
        pltpu.make_async_copy(ref, target, down_sems.at[index])
        for index, (ref, target) in enumerate(zip(sources, targets))
    ]
    hidden_ref[...] = stream_hidden(row_refs, weight_refs, *scratch, later=loads)
    loads[0].wait()
    first = first_rows[early_rows:]
    second = hidden_ref[early_rows:]
    col = 0
    for load, weight in zip(loads[1:], (down_own, down_near)):
        load.wait()
        total = down_rows(place_ref[0], first, second, weight)
        row = 0
        for ref in out_refs:
            ref[:, col : col + total.shape[1]] = total[row : row + ref.shape[0]]
            row += ref.shape[0]
        col += total.shape[1]


def second_hidden(place, first, row_parts, weights, downs, sizes, early):
    rows = sum(sizes)
    width = weights[0].shape[1] * len(weights) // 2
    out_width = 2 * downs[0].shape[1]
    outs = [jax.ShapeDtypeStruct((rows, width), jnp.bfloat16)]
    outs += [jax.ShapeDtypeStruct((sizes[k], out_width), jnp.bfloat16) for k in early]
    hidden, *results = pl.pallas_call(
        functools.partial(second_kernel, len(row_parts), len(weights), sum(sizes[: early[0]])),
        out_shape=outs,
        in_specs=[SMEM, ANY] + [ANY] * (len(row_parts) + len(weights) + 2),
        out_specs=[VMEM] * len(outs),
        scratch_shapes=[
            pltpu.VMEM(first.shape, jnp.bfloat16),
            pltpu.VMEM(downs[0].shape, jnp.bfloat16),
            pltpu.VMEM(downs[1].shape, jnp.bfloat16),
            pltpu.SemaphoreType.DMA((3,)),
        ]
        + hidden_scratch(row_parts, weights),
        compiler_params=pltpu.CompilerParams(vmem_limit_bytes=56 * MIB),
        cost_estimate=pl.CostEstimate(flops=MIB, bytes_accessed=MIB, transcendentals=0),
        name="second_hidden",
    )(place, first, *row_parts, *weights, *downs)
    return hidden, dict(zip(early, results))


def late_kernel(far, sizes, early, place_ref, *refs):
    first_ref, second_ref, first_far_ref, second_far_ref, own_ref, near_ref, *refs = refs
    out_refs, (down_own, down_near, sems) = refs[:-3], refs[-3:]
    loads = [
        pltpu.make_async_copy(own_ref, down_own, sems.at[0]),
        pltpu.make_async_copy(near_ref, down_near, sems.at[1]),
    ]
    for load in loads:
        load.start()
    later = [k for k in range(len(sizes)) if k not in early]
    own_rows = sum(sizes[k] for k in later)
    col = 0
    for load, weight_ref in zip(loads, (down_own, down_near)):
        load.wait()
        total = down_rows(place_ref[0] ^ far, first_far_ref[...], second_far_ref[...], weight_ref)
        width = total.shape[1]
        row = 0
        for k, ref in enumerate(out_refs):
            at = 0 if k in early else sizes[k]
            ref[at:, col : col + width] = total[row : row + sizes[k]]
            row += sizes[k]
        if later:
            total = down_rows(place_ref[0], first_ref[:own_rows], second_ref[:own_rows], weight_ref)
            row = 0
            for k in later:
                out_refs[k][: sizes[k], col : col + width] = total[row : row + sizes[k]]
                row += sizes[k]
        col += width


def late_results(place, far, hidden_parts, downs, sizes, early):
    out_width = 2 * downs[0].shape[1]
    rows = [sizes[k] if k in early else 2 * sizes[k] for k in range(len(sizes))]
    return pl.pallas_call(
        functools.partial(late_kernel, far, tuple(sizes), tuple(early)),
        out_shape=[pltpu.HBM((count, out_width), jnp.bfloat16) for count in rows],
        in_specs=[SMEM] + [VMEM] * 4 + [ANY] * 2,
        out_specs=[VMEM] * len(rows),
        scratch_shapes=[
            pltpu.VMEM(downs[0].shape, jnp.bfloat16),
            pltpu.VMEM(downs[1].shape, jnp.bfloat16),
            pltpu.SemaphoreType.DMA((2,)),
        ],
        compiler_params=pltpu.CompilerParams(vmem_limit_bytes=24 * MIB),
        cost_estimate=pl.CostEstimate(
            flops=2 * sum(rows) * downs[0].shape[0] * out_width,
            bytes_accessed=4 * MIB,
            transcendentals=0,
        ),
        name="late_down",
    )(place, *hidden_parts, *downs)


def front_kernel(place_ref, *refs):
    part_refs, weight_refs, refs = refs[:4], refs[4:7], refs[7:]
    product_ref, gate_ref, rows, weights, row_sems, weight_sems = refs
    tok = part_refs[0].shape[0]
    copies = []
    for j, ref in enumerate(part_refs):
        start = pl.multiple_of((place_ref[0] ^ j) * tok, tok)
        copies.append(pltpu.make_async_copy(ref, rows.at[pl.ds(start, tok)], row_sems.at[j]))
    loads = [
        pltpu.make_async_copy(ref, weights.at[index], weight_sems.at[index])
        for index, ref in enumerate(weight_refs)
    ]
    for copy in copies + loads[:1]:
        copy.start()
    for copy in copies:
        copy.wait()
    loads[1].start()
    loads[0].wait()
    loads[2].start()
    in_gate = jnp.dot(rows[...], weights[0], preferred_element_type=jnp.float32)
    loads[1].wait()
    values = jnp.dot(rows[...], weights[1], preferred_element_type=jnp.float32)
    product_ref[...] = (in_gate * values).astype(jnp.bfloat16)
    loads[2].wait()
    gate_ref[...] = jnp.dot(rows[...], weights[2], preferred_element_type=jnp.float32)


def mixer_front(place, parts, weights):
    rows = sum(part.shape[0] for part in parts)
    depth, width = weights[0].shape
    return pl.pallas_call(
        front_kernel,
        out_shape=[
            jax.ShapeDtypeStruct((rows, width), jnp.bfloat16),
            jax.ShapeDtypeStruct((rows, width), jnp.float32),
        ],
        in_specs=[SMEM] + [ANY] * 7,
        out_specs=[VMEM, VMEM],
        scratch_shapes=[
            pltpu.VMEM((rows, depth), jnp.bfloat16),
            pltpu.VMEM((3, depth, width), jnp.bfloat16),
            pltpu.SemaphoreType.DMA((4,)),
            pltpu.SemaphoreType.DMA((3,)),
        ],
        compiler_params=pltpu.CompilerParams(vmem_limit_bytes=56 * MIB),
        cost_estimate=pl.CostEstimate(
            flops=6 * rows * depth * width, bytes_accessed=8 * MIB, transcendentals=0
        ),
        name="mixer_front",
    )(place, *parts, *weights)


def share_masks(mask, hits, share_rows):
    share_of = jnp.sum(jnp.where(hits, share_rows[:, None, :], 0.0), axis=0)
    mixed = jnp.where(mask, share_of[:, None, :], 0.0).reshape(-1, mask.shape[2])
    high = mixed.astype(jnp.bfloat16)
    return high, (mixed - high.astype(jnp.float32)).astype(jnp.bfloat16)


def combine_rows(masks, returned):
    dims = (((0,), (0,)), ((), ()))
    total = lax.dot_general(masks[0], returned, dims, preferred_element_type=jnp.float32)
    total = total + lax.dot_general(masks[1], returned, dims, preferred_element_type=jnp.float32)
    return total


def on_device(
    mixer_in,
    expert_in,
    mixer_gain,
    in_gate_weight,
    out_gate_weight,
    value_weight,
    conv_taps,
    mixer_proj,
    expert_gain,
    route_ids,
    route_weights,
    gate_weight,
    up_weight,
    down_weight,
):
    tok_dev = mixer_in.shape[0]
    tp_count = lax.axis_size("tp")
    ep_count = lax.axis_size("ep")
    top_count = route_ids.shape[1]
    experts = ep_count * gate_weight.shape[0]
    slot_cap = max(2, 2 * tok_dev * top_count // experts)
    tp_index = lax.axis_index("tp")
    ep_index = lax.axis_index("ep")
    direct = swaps_direct(ep_count)
    near, far = 1, tp_count // 2

    gates, ups = {0: gate_weight[0]}, {0: up_weight[0]}
    gates[far] = swapped(gates[0], "tp", far)
    ups[far] = swapped(ups[0], "tp", far)
    gates[near] = swapped(gates[0], "tp", near)
    ups[near] = swapped(ups[0], "tp", near)
    down_own = down_weight[0]
    down_near = swapped(down_own, "tp", near)
    order = [0, near, far, far ^ near]

    def rows_of(weight, j, width):
        return lax.dynamic_slice_in_dim(weight, (tp_index ^ j) * width, width, 0)

    peers = jnp.arange(experts, dtype=jnp.int32)
    labels = (peers ^ ep_index) if direct else peers

    def block_of(values, j):
        return lax.dynamic_slice_in_dim(values, (tp_index ^ j) * tok_dev, tok_dev, 0)

    hits_own, mask_own = slot_masks(block_of(route_ids, 0).T, labels, slot_cap)
    hits_far, mask_far = slot_masks(block_of(route_ids, far).T, labels, slot_cap)
    shares = route_weights / jnp.sum(route_weights, axis=1, keepdims=True)
    masks_own = share_masks(mask_own, hits_own, block_of(shares, 0).T)
    masks_far = share_masks(mask_far, hits_far, block_of(shares, far).T)
    chan_width = in_gate_weight.shape[1]
    tap_count = conv_taps.shape[0]
    tap_rows = lax.dynamic_slice_in_dim(conv_taps, tp_index * chan_width, chan_width, 1)
    tap_rows = [tap_rows[tap_index] for tap_index in range(tap_count)]
    mixer_normed = rms_rows(mixer_in, mixer_gain)
    place = jnp.where(jnp.arange(2) == 0, tp_index, ep_index).astype(jnp.int32)
    sizes = [slot_cap] * experts if direct else [experts * slot_cap]
    early = list(range(len(sizes) // 2, len(sizes)))
    outgoing = dispatched(
        place, route_ids.T, expert_in, expert_gain[None, :], sizes, direct, slot_cap
    )
    arrived = exchange(dict(enumerate(outgoing)), "ep", direct)
    gates[far ^ near] = swapped(gates[far], "tp", near)
    ready = (masks_own, masks_far, mixer_normed, gates[far ^ near])
    ready += (gates[near], ups[near], down_near)
    arrived[0] = after(arrived[0], *ready)
    slots_in = [arrived[k] for k in range(len(sizes))]

    first = first_hidden(slots_in, [half[j] for j in (0, near) for half in (gates, ups)])
    ups[far ^ near] = swapped(after(ups[far], first), "tp", near)
    downs = (down_own, down_near)
    second, done_own = second_hidden(
        place,
        first,
        slots_in,
        [half[j] for j in (far, far ^ near) for half in (gates, ups)],
        downs,
        sizes,
        early,
    )
    first_far = swapped(after(first, ups[far]), "tp", far)
    second_far = swapped(second, "tp", far)
    back_own = exchange(done_own, "ep", direct)

    normed = {0: after(mixer_normed, ups[far], first)}
    normed[far] = swapped(normed[0], "tp", far)
    normed[near] = swapped(normed[0], "tp", near)
    normed = {j: after(normed[j], second) for j in normed}
    normed[far ^ near] = swapped(normed[far], "tp", near)
    product, out_gate = mixer_front(
        place, [normed[j] for j in order], [in_gate_weight, value_weight, out_gate_weight]
    )
    row_count = product.shape[0]
    rim_rows = lax.ppermute(
        product[row_count - (tap_count - 1) :], "ep", [(i, i + 1) for i in range(ep_count - 1)]
    )
    extended = jnp.concatenate([rim_rows, product], axis=0).astype(jnp.float32)
    conv_sum = tap_rows[0] * extended[0:row_count]
    for tap_index in range(1, tap_count):
        conv_sum = conv_sum + tap_rows[tap_index] * extended[tap_index : tap_index + row_count]
    gated = {0: (out_gate * conv_sum).astype(jnp.bfloat16)}
    gated[far] = swapped(gated[0], "tp", far)
    gated[near] = swapped(gated[0], "tp", near)
    gated[far ^ near] = swapped(gated[far], "tp", near)
    mixer_sum = None
    for j in order:
        term = jnp.dot(
            gated[j], rows_of(mixer_proj, j, chan_width), preferred_element_type=jnp.float32
        )
        mixer_sum = term if mixer_sum is None else mixer_sum + term
    first_far = after(first_far, product)
    late = late_results(place, far, (first, second, first_far, second_far), downs, sizes, early)
    back_late = exchange(dict(enumerate(late)), "ep", direct)
    width = slot_cap if direct else sizes[0]
    later = [k for k in range(len(sizes)) if k not in early]
    own_early = combine_rows(
        [mask[early[0] * width :] for mask in masks_own],
        jnp.concatenate([back_own[k] for k in early], axis=0),
    )
    back_late[0] = after(back_late[0], mixer_sum, own_early)
    far_rows = [back_late[k][-sizes[k] :] for k in range(len(sizes))]
    mixed_own = own_early
    if later:
        own_rows = [back_late[k][: sizes[k]] for k in later]
        masks_later = [mask[: len(later) * width] for mask in masks_own]
        mixed_own = mixed_own + combine_rows(masks_later, jnp.concatenate(own_rows, axis=0))
    mixed_own = mixed_own.astype(jnp.bfloat16)
    mixed_far = combine_rows(masks_far, jnp.concatenate(far_rows, axis=0)).astype(jnp.bfloat16)
    mixed = jnp.concatenate([mixed_own, mixed_far], axis=0)
    col_width = down_own.shape[1]
    mixed_near = swapped(mixed[:, col_width:], "tp", near)
    expert_out = jnp.zeros((tp_count * tok_dev, col_width), jnp.bfloat16)
    for j, block in (
        (0, mixed[:tok_dev, :col_width]),
        (far, mixed[tok_dev:, :col_width]),
        (near, mixed_near[:tok_dev]),
        (far ^ near, mixed_near[tok_dev:]),
    ):
        expert_out = lax.dynamic_update_slice_in_dim(
            expert_out, block, (tp_index ^ j) * tok_dev, 0
        )

    return (mixer_sum.astype(jnp.bfloat16), expert_out)


def solution(mesh):
    return jax.shard_map(
        on_device,
        mesh=mesh,
        in_specs=(
            P(("ep", "tp"), None),
            P(("ep", "tp"), None),
            P(),
            P(None, "tp"),
            P(None, "tp"),
            P(None, "tp"),
            P(),
            P(None, "tp"),
            P(),
            P("ep", None),
            P("ep", None),
            P("ep", None, "tp"),
            P("ep", None, "tp"),
            P("ep", None, "tp"),
        ),
        out_specs=(P("ep", "tp"), P("ep", "tp")),
        check_vma=False,
    )
```

```python
import functools

import jax
import jax.numpy as jnp
from jax import lax
from jax.experimental import pallas as pl
from jax.experimental.pallas import tpu as pltpu
from jax.sharding import PartitionSpec as P


norm_eps = 1e-06


def rms_rows(values, gain_row):
    wide = values.astype(jnp.float32)
    scale = lax.rsqrt(jnp.mean(wide * wide, axis=-1, keepdims=True) + norm_eps)
    return (wide * scale * gain_row).astype(jnp.bfloat16)


def swapped(value, axis, mask):
    count = lax.axis_size(axis)
    return lax.ppermute(value, axis, [(source, source ^ mask) for source in range(count)])


def after(value, *earlier):
    return lax.optimization_barrier((value, earlier))[0]


def slot_masks(block_ids, labels, slot_cap):
    rows = block_ids.shape[1]
    hits = block_ids[:, None, :] == labels[None, :, None]
    member = jnp.any(hits, axis=0)
    order = jnp.arange(rows, dtype=jnp.int32)
    before = (order[:, None] < order[None, :]).astype(jnp.bfloat16)
    rank = jnp.dot(member.astype(jnp.bfloat16), before, preferred_element_type=jnp.float32)
    rank = jnp.where(member, rank, -1.0)
    slots = jnp.arange(slot_cap, dtype=jnp.int32).astype(jnp.float32)
    return hits, rank[:, None, :] == slots[None, :, None]


def swaps_direct(count):
    return count <= 16 and count & (count - 1) == 0


def start_order(count):
    across = [k for k in range(1, count) if k & (count // 2)]
    nearer = [k for k in range(2, count // 2)]
    half = len(across) // 2
    return across[:half] + [1] * (count > 2) + nearer + across[half:]


def exchange(chunks, axis, direct):
    if direct:
        moved = dict(chunks)
        for k in start_order(lax.axis_size(axis)):
            if k in chunks:
                moved[k] = swapped(chunks[k], axis, k)
        return moved
    rows = chunks[0]
    split = rows.reshape(lax.axis_size(axis), -1, rows.shape[1])
    moved = lax.all_to_all(split, axis, split_axis=0, concat_axis=0, tiled=True)
    return {0: moved.reshape(rows.shape)}


MIB = 1 << 20
STREAMS = 4
ANY = pl.BlockSpec(memory_space=pl.ANY)
VMEM = pl.BlockSpec(memory_space=pltpu.VMEM)
SMEM = pl.BlockSpec(memory_space=pltpu.SMEM)


def dispatch_kernel(direct, slot_cap, place_ref, ids_ref, source_ref, gain_ref, *refs):
    out_refs, (rows_ref, sem) = refs[:-2], refs[-2:]
    load = pltpu.make_async_copy(source_ref, rows_ref, sem)
    load.start()
    tok, width = rows_ref.shape
    total = ids_ref.shape[1]
    slots = sum(ref.shape[0] for ref in out_refs)
    experts = slots // slot_cap
    lanes = min(total, -(-tok // 128) * 128)
    tp_index, ep_index = place_ref[0], place_ref[1]
    ids = pltpu.roll(ids_ref[...], lax.rem(total - tp_index * tok, total), 1)[:, :lanes]
    labels = lax.broadcasted_iota(jnp.int32, (experts, lanes), 0)
    if direct:
        labels = labels ^ ep_index
    member = ids[0:1] == labels
    for pick in range(1, ids_ref.shape[0]):
        member = member | (ids[pick : pick + 1] == labels)
    first = lax.broadcasted_iota(jnp.int32, (lanes, lanes), 0)
    second = lax.broadcasted_iota(jnp.int32, (lanes, lanes), 1)
    before = jnp.where(first < second, 1.0, 0.0).astype(jnp.bfloat16)
    member = jnp.where(member, 1.0, 0.0)
    rank = jnp.dot(member.astype(jnp.bfloat16), before, preferred_element_type=jnp.float32)
    rank = jnp.where(member > 0.5, rank, -1.0).astype(jnp.bfloat16)
    slot = lax.broadcasted_iota(jnp.int32, (slots, experts), 0)
    start = lax.broadcasted_iota(jnp.int32, (slots, experts), 1) * slot_cap
    inside = (slot >= start) & (slot < start + slot_cap)
    spread = jnp.where(inside, 1.0, 0.0)
    rank_of = jnp.dot(spread.astype(jnp.bfloat16), rank, preferred_element_type=jnp.float32)
    offset = jnp.where(inside, (slot - start).astype(jnp.float32), 0.0)
    offset = jnp.sum(offset, axis=1, keepdims=True)
    mask = jnp.where(rank_of == offset, 1.0, 0.0)[:, :tok].astype(jnp.bfloat16)
    load.wait()
    wide = rows_ref[...].astype(jnp.float32)
    scale = lax.rsqrt(jnp.mean(wide * wide, axis=-1, keepdims=True) + norm_eps)
    normed = (wide * scale * gain_ref[...]).astype(jnp.bfloat16)
    step = min(width, 512)
    for col in range(0, width, step):
        part = jnp.dot(mask, normed[:, col : col + step], preferred_element_type=jnp.float32)
        part = part.astype(jnp.bfloat16)
        row = 0
        for ref in out_refs:
            ref[:, col : col + step] = part[row : row + ref.shape[0]]
            row += ref.shape[0]


def dispatched(place, ids, rows, gain, sizes, direct, slot_cap):
    width = rows.shape[1]
    return pl.pallas_call(
        functools.partial(dispatch_kernel, direct, slot_cap),
        out_shape=[jax.ShapeDtypeStruct((size, width), jnp.bfloat16) for size in sizes],
        in_specs=[SMEM, VMEM, ANY, VMEM],
        out_specs=[VMEM] * len(sizes),
        scratch_shapes=[pltpu.VMEM(rows.shape, rows.dtype), pltpu.SemaphoreType.DMA],
        compiler_params=pltpu.CompilerParams(vmem_limit_bytes=56 * MIB),
        cost_estimate=pl.CostEstimate(
            flops=2 * sum(sizes) * rows.shape[0] * width, bytes_accessed=2 * MIB, transcendentals=0
        ),
        name="dispatch",
    )(place, ids, rows, gain)


def stream_hidden(row_refs, weight_refs, rows, weights, row_sems, weight_sems, later=()):
    chunks = row_sems.shape[0]
    depth = rows.shape[1] // chunks
    plan = []
    for chunk in range(chunks):
        part = pl.ds(chunk * depth, depth)
        copies, row = [], 0
        for index, ref in enumerate(row_refs):
            target = rows.at[pl.ds(row, ref.shape[0]), part]
            sem = row_sems.at[chunk, index]
            copies.append(pltpu.make_async_copy(ref.at[:, part], target, sem))
            row += ref.shape[0]
        for index, ref in enumerate(weight_refs):
            width = ref.shape[1]
            target = weights.at[index % 2, part, pl.ds(index // 2 * width, width)]
            sem = weight_sems.at[chunk, index]
            copies.append(pltpu.make_async_copy(ref.at[part, :], target, sem))
        for copy in copies:
            copy.start()
        plan.append(copies)
    gate_pre = up_pre = None
    for chunk in range(chunks):
        for copy in plan[chunk]:
            copy.wait()
        if chunk == 0:
            for copy in later:
                copy.start()
        part = slice(chunk * depth, (chunk + 1) * depth)
        here = rows[:, part]
        gate_term = jnp.dot(here, weights[0, part, :], preferred_element_type=jnp.float32)
        up_term = jnp.dot(here, weights[1, part, :], preferred_element_type=jnp.float32)
        gate_pre = gate_term if gate_pre is None else gate_pre + gate_term
        up_pre = up_term if up_pre is None else up_pre + up_term
    return (gate_pre / (1.0 + jnp.exp(-gate_pre)) * up_pre).astype(jnp.bfloat16)


def hidden_scratch(row_parts, weights):
    rows = sum(part.shape[0] for part in row_parts)
    depth, width = weights[0].shape
    return [
        pltpu.VMEM((rows, depth), jnp.bfloat16),
        pltpu.VMEM((2, depth, width * len(weights) // 2), jnp.bfloat16),
        pltpu.SemaphoreType.DMA((STREAMS, len(row_parts))),
        pltpu.SemaphoreType.DMA((STREAMS, len(weights))),
    ]


def hidden_cost(row_parts, weights):
    rows = sum(part.shape[0] for part in row_parts)
    depth, width = weights[0].shape
    return pl.CostEstimate(
        flops=2 * rows * depth * width * len(weights),
        bytes_accessed=2 * (rows * depth + len(weights) * depth * width),
        transcendentals=rows * width * len(weights) // 2,
    )


def first_kernel(row_count, *refs):
    row_refs, refs = refs[:row_count], refs[row_count:]
    weight_refs, (out_ref, *scratch) = refs[:-5], refs[-5:]
    out_ref[...] = stream_hidden(row_refs, weight_refs, *scratch)


def first_hidden(row_parts, weights):
    rows = sum(part.shape[0] for part in row_parts)
    width = weights[0].shape[1] * len(weights) // 2
    return pl.pallas_call(
        functools.partial(first_kernel, len(row_parts)),
        out_shape=jax.ShapeDtypeStruct((rows, width), jnp.bfloat16),
        in_specs=[ANY] * (len(row_parts) + len(weights)),
        out_specs=VMEM,
        scratch_shapes=hidden_scratch(row_parts, weights),
        compiler_params=pltpu.CompilerParams(vmem_limit_bytes=56 * MIB),
        cost_estimate=hidden_cost(row_parts, weights),
        name="first_hidden",
    )(*row_parts, *weights)


def down_rows(place, first, second, weight_ref):
    half = first.shape[1] // 2
    total = None
    for j in range(4):
        source = first if j < 2 else second
        block = source[:, (j % 2) * half : (j % 2 + 1) * half]
        start = pl.multiple_of((place ^ j) * half, half)
        term = jnp.dot(block, weight_ref[pl.ds(start, half), :], preferred_element_type=jnp.float32)
        total = term if total is None else total + term
    return total.astype(jnp.bfloat16)


def second_kernel(row_count, weight_count, early_rows, place_ref, first_ref, *refs):
    row_refs, refs = refs[:row_count], refs[row_count:]
    weight_refs, refs = refs[:weight_count], refs[weight_count:]
    down_refs, (hidden_ref, *refs) = refs[:2], refs[2:]
    out_refs, (first_rows, down_own, down_near, down_sems, *scratch) = refs[:-8], refs[-8:]
    sources, targets = (first_ref, *down_refs), (first_rows, down_own, down_near)
    loads = [
        pltpu.make_async_copy(ref, target, down_sems.at[index])
        for index, (ref, target) in enumerate(zip(sources, targets))
    ]
    hidden_ref[...] = stream_hidden(row_refs, weight_refs, *scratch, later=loads)
    loads[0].wait()
    first = first_rows[early_rows:]
    second = hidden_ref[early_rows:]
    col = 0
    for load, weight in zip(loads[1:], (down_own, down_near)):
        load.wait()
        total = down_rows(place_ref[0], first, second, weight)
        row = 0
        for ref in out_refs:
            ref[:, col : col + total.shape[1]] = total[row : row + ref.shape[0]]
            row += ref.shape[0]
        col += total.shape[1]


def second_hidden(place, first, row_parts, weights, downs, sizes, early):
    rows = sum(sizes)
    width = weights[0].shape[1] * len(weights) // 2
    out_width = 2 * downs[0].shape[1]
    outs = [jax.ShapeDtypeStruct((rows, width), jnp.bfloat16)]
    outs += [jax.ShapeDtypeStruct((sizes[k], out_width), jnp.bfloat16) for k in early]
    hidden, *results = pl.pallas_call(
        functools.partial(second_kernel, len(row_parts), len(weights), sum(sizes[: early[0]])),
        out_shape=outs,
        in_specs=[SMEM, ANY] + [ANY] * (len(row_parts) + len(weights) + 2),
        out_specs=[VMEM] * len(outs),
        scratch_shapes=[
            pltpu.VMEM(first.shape, jnp.bfloat16),
            pltpu.VMEM(downs[0].shape, jnp.bfloat16),
            pltpu.VMEM(downs[1].shape, jnp.bfloat16),
            pltpu.SemaphoreType.DMA((3,)),
        ]
        + hidden_scratch(row_parts, weights),
        compiler_params=pltpu.CompilerParams(vmem_limit_bytes=56 * MIB),
        cost_estimate=pl.CostEstimate(flops=MIB, bytes_accessed=MIB, transcendentals=0),
        name="second_hidden",
    )(place, first, *row_parts, *weights, *downs)
    return hidden, dict(zip(early, results))


def late_kernel(far, sizes, early, place_ref, *refs):
    first_ref, second_ref, first_far_ref, second_far_ref, own_ref, near_ref, *refs = refs
    out_refs, (down_own, down_near, sems) = refs[:-3], refs[-3:]
    loads = [
        pltpu.make_async_copy(own_ref, down_own, sems.at[0]),
        pltpu.make_async_copy(near_ref, down_near, sems.at[1]),
    ]
    for load in loads:
        load.start()
    later = [k for k in range(len(sizes)) if k not in early]
    own_rows = sum(sizes[k] for k in later)
    col = 0
    for load, weight_ref in zip(loads, (down_own, down_near)):
        load.wait()
        total = down_rows(place_ref[0] ^ far, first_far_ref[...], second_far_ref[...], weight_ref)
        width = total.shape[1]
        row = 0
        for k, ref in enumerate(out_refs):
            at = 0 if k in early else sizes[k]
            ref[at:, col : col + width] = total[row : row + sizes[k]]
            row += sizes[k]
        if later:
            total = down_rows(place_ref[0], first_ref[:own_rows], second_ref[:own_rows], weight_ref)
            row = 0
            for k in later:
                out_refs[k][: sizes[k], col : col + width] = total[row : row + sizes[k]]
                row += sizes[k]
        col += width


def late_results(place, far, hidden_parts, downs, sizes, early):
    out_width = 2 * downs[0].shape[1]
    rows = [sizes[k] if k in early else 2 * sizes[k] for k in range(len(sizes))]
    return pl.pallas_call(
        functools.partial(late_kernel, far, tuple(sizes), tuple(early)),
        out_shape=[pltpu.HBM((count, out_width), jnp.bfloat16) for count in rows],
        in_specs=[SMEM] + [VMEM] * 4 + [ANY] * 2,
        out_specs=[VMEM] * len(rows),
        scratch_shapes=[
            pltpu.VMEM(downs[0].shape, jnp.bfloat16),
            pltpu.VMEM(downs[1].shape, jnp.bfloat16),
            pltpu.SemaphoreType.DMA((2,)),
        ],
        compiler_params=pltpu.CompilerParams(vmem_limit_bytes=24 * MIB),
        cost_estimate=pl.CostEstimate(
            flops=2 * sum(rows) * downs[0].shape[0] * out_width,
            bytes_accessed=4 * MIB,
            transcendentals=0,
        ),
        name="late_down",
    )(place, *hidden_parts, *downs)


def front_kernel(place_ref, *refs):
    part_refs, weight_refs, refs = refs[:4], refs[4:7], refs[7:]
    product_ref, gate_ref, rim_ref, rows, weights, row_sems, weight_sems = refs
    tok = part_refs[0].shape[0]
    copies = []
    for j, ref in enumerate(part_refs):
        start = pl.multiple_of((place_ref[0] ^ j) * tok, tok)
        copies.append(pltpu.make_async_copy(ref, rows.at[pl.ds(start, tok)], row_sems.at[j]))
    loads = [
        pltpu.make_async_copy(ref, weights.at[index], weight_sems.at[index])
        for index, ref in enumerate(weight_refs)
    ]
    for copy in copies + loads[:1]:
        copy.start()
    for copy in copies:
        copy.wait()
    loads[1].start()
    loads[0].wait()
    loads[2].start()
    in_gate = jnp.dot(rows[...], weights[0], preferred_element_type=jnp.float32)
    loads[1].wait()
    values = jnp.dot(rows[...], weights[1], preferred_element_type=jnp.float32)
    product = (in_gate * values).astype(jnp.bfloat16)
    product_ref[...] = product
    rim_ref[...] = product[product.shape[0] - rim_ref.shape[0] :]
    loads[2].wait()
    gate_ref[...] = jnp.dot(rows[...], weights[2], preferred_element_type=jnp.float32)


def mixer_front(place, parts, weights, rim):
    rows = sum(part.shape[0] for part in parts)
    depth, width = weights[0].shape
    return pl.pallas_call(
        front_kernel,
        out_shape=[
            jax.ShapeDtypeStruct((rows, width), jnp.bfloat16),
            jax.ShapeDtypeStruct((rows, width), jnp.float32),
            jax.ShapeDtypeStruct((rim, width), jnp.bfloat16),
        ],
        in_specs=[SMEM] + [ANY] * 7,
        out_specs=[VMEM, VMEM, VMEM],
        scratch_shapes=[
            pltpu.VMEM((rows, depth), jnp.bfloat16),
            pltpu.VMEM((3, depth, width), jnp.bfloat16),
            pltpu.SemaphoreType.DMA((4,)),
            pltpu.SemaphoreType.DMA((3,)),
        ],
        compiler_params=pltpu.CompilerParams(vmem_limit_bytes=56 * MIB),
        cost_estimate=pl.CostEstimate(
            flops=6 * rows * depth * width, bytes_accessed=8 * MIB, transcendentals=0
        ),
        name="mixer_front",
    )(place, *parts, *weights)


def share_masks(mask, hits, share_rows):
    share_of = jnp.sum(jnp.where(hits, share_rows[:, None, :], 0.0), axis=0)
    mixed = jnp.where(mask, share_of[:, None, :], 0.0).reshape(-1, mask.shape[2])
    high = mixed.astype(jnp.bfloat16)
    return high, (mixed - high.astype(jnp.float32)).astype(jnp.bfloat16)


def combine_rows(masks, returned):
    dims = (((0,), (0,)), ((), ()))
    total = lax.dot_general(masks[0], returned, dims, preferred_element_type=jnp.float32)
    total = total + lax.dot_general(masks[1], returned, dims, preferred_element_type=jnp.float32)
    return total


def on_device(
    mixer_in,
    expert_in,
    mixer_gain,
    in_gate_weight,
    out_gate_weight,
    value_weight,
    conv_taps,
    mixer_proj,
    expert_gain,
    route_ids,
    route_weights,
    gate_weight,
    up_weight,
    down_weight,
):
    tok_dev = mixer_in.shape[0]
    tp_count = lax.axis_size("tp")
    ep_count = lax.axis_size("ep")
    top_count = route_ids.shape[1]
    experts = ep_count * gate_weight.shape[0]
    slot_cap = max(2, 2 * tok_dev * top_count // experts)
    tp_index = lax.axis_index("tp")
    ep_index = lax.axis_index("ep")
    direct = swaps_direct(ep_count)
    near, far = 1, tp_count // 2

    gates, ups = {0: gate_weight[0]}, {0: up_weight[0]}
    gates[far] = swapped(gates[0], "tp", far)
    ups[far] = swapped(ups[0], "tp", far)
    gates[near] = swapped(gates[0], "tp", near)
    ups[near] = swapped(ups[0], "tp", near)
    down_own = down_weight[0]
    down_near = swapped(down_own, "tp", near)
    order = [0, near, far, far ^ near]

    def rows_of(weight, j, width):
        return lax.dynamic_slice_in_dim(weight, (tp_index ^ j) * width, width, 0)

    peers = jnp.arange(experts, dtype=jnp.int32)
    labels = (peers ^ ep_index) if direct else peers

    def block_of(values, j):
        return lax.dynamic_slice_in_dim(values, (tp_index ^ j) * tok_dev, tok_dev, 0)

    hits_own, mask_own = slot_masks(block_of(route_ids, 0).T, labels, slot_cap)
    hits_far, mask_far = slot_masks(block_of(route_ids, far).T, labels, slot_cap)
    shares = route_weights / jnp.sum(route_weights, axis=1, keepdims=True)
    masks_own = share_masks(mask_own, hits_own, block_of(shares, 0).T)
    masks_far = share_masks(mask_far, hits_far, block_of(shares, far).T)
    chan_width = in_gate_weight.shape[1]
    tap_count = conv_taps.shape[0]
    tap_rows = lax.dynamic_slice_in_dim(conv_taps, tp_index * chan_width, chan_width, 1)
    tap_rows = [tap_rows[tap_index] for tap_index in range(tap_count)]
    mixer_normed = rms_rows(mixer_in, mixer_gain)
    place = jnp.where(jnp.arange(2) == 0, tp_index, ep_index).astype(jnp.int32)
    sizes = [slot_cap] * experts if direct else [experts * slot_cap]
    early = list(range(len(sizes) // 2, len(sizes)))
    outgoing = dispatched(
        place, route_ids.T, expert_in, expert_gain[None, :], sizes, direct, slot_cap
    )
    arrived = exchange(dict(enumerate(outgoing)), "ep", direct)
    gates[far ^ near] = swapped(gates[far], "tp", near)
    ready = (masks_own, masks_far, mixer_normed, gates[far ^ near])
    ready += (gates[near], ups[near], down_near)
    ready += tuple(tap_rows)
    arrived[0] = after(arrived[0], *ready)
    slots_in = [arrived[k] for k in range(len(sizes))]

    first = first_hidden(slots_in, [half[j] for j in (0, near) for half in (gates, ups)])
    ups[far ^ near] = swapped(after(ups[far], first), "tp", near)
    downs = (down_own, down_near)
    second, done_own = second_hidden(
        place,
        first,
        slots_in,
        [half[j] for j in (far, far ^ near) for half in (gates, ups)],
        downs,
        sizes,
        early,
    )
    first_far = swapped(after(first, ups[far]), "tp", far)
    second_far = swapped(second, "tp", far)
    back_own = exchange(done_own, "ep", direct)

    normed = {0: mixer_normed}
    normed[far] = swapped(normed[0], "tp", far)
    normed[near] = swapped(normed[0], "tp", near)
    normed = {j: after(normed[j], second) for j in normed}
    normed[far ^ near] = swapped(normed[far], "tp", near)
    front_weights = [in_gate_weight, value_weight, out_gate_weight]
    product, out_gate, rim_sent = mixer_front(
        place, [normed[j] for j in order], front_weights, tap_count - 1
    )
    row_count = product.shape[0]
    steps = [(source, source + 1) for source in range(ep_count - 1)]
    rim_rows = lax.ppermute(rim_sent, "ep", steps)
    extended = jnp.concatenate([rim_rows, product], axis=0).astype(jnp.float32)
    conv_sum = tap_rows[0] * extended[0:row_count]
    for tap_index in range(1, tap_count):
        conv_sum = conv_sum + tap_rows[tap_index] * extended[tap_index : tap_index + row_count]
    gated = {0: (out_gate * conv_sum).astype(jnp.bfloat16)}
    gated[far] = swapped(gated[0], "tp", far)
    gated[near] = swapped(gated[0], "tp", near)
    gated[far ^ near] = swapped(gated[far], "tp", near)
    mixer_sum = None
    for j in order:
        term = jnp.dot(
            gated[j], rows_of(mixer_proj, j, chan_width), preferred_element_type=jnp.float32
        )
        mixer_sum = term if mixer_sum is None else mixer_sum + term
    first_far = after(first_far, product)
    late = late_results(place, far, (first, second, first_far, second_far), downs, sizes, early)
    back_late = exchange(dict(enumerate(late)), "ep", direct)
    width = slot_cap if direct else sizes[0]
    later = [k for k in range(len(sizes)) if k not in early]
    own_early = combine_rows(
        [mask[early[0] * width :] for mask in masks_own],
        jnp.concatenate([back_own[k] for k in early], axis=0),
    )
    back_late[0] = after(back_late[0], mixer_sum, own_early)
    far_rows = [back_late[k][-sizes[k] :] for k in range(len(sizes))]
    mixed_own = own_early
    if later:
        own_rows = [back_late[k][: sizes[k]] for k in later]
        masks_later = [mask[: len(later) * width] for mask in masks_own]
        mixed_own = mixed_own + combine_rows(masks_later, jnp.concatenate(own_rows, axis=0))
    mixed_own = mixed_own.astype(jnp.bfloat16)
    mixed_far = combine_rows(masks_far, jnp.concatenate(far_rows, axis=0)).astype(jnp.bfloat16)
    mixed = jnp.concatenate([mixed_own, mixed_far], axis=0)
    col_width = down_own.shape[1]
    mixed_near = swapped(mixed[:, col_width:], "tp", near)
    expert_out = jnp.zeros((tp_count * tok_dev, col_width), jnp.bfloat16)
    for j, block in (
        (0, mixed[:tok_dev, :col_width]),
        (far, mixed[tok_dev:, :col_width]),
        (near, mixed_near[:tok_dev]),
        (far ^ near, mixed_near[tok_dev:]),
    ):
        expert_out = lax.dynamic_update_slice_in_dim(
            expert_out, block, (tp_index ^ j) * tok_dev, 0
        )

    return (mixer_sum.astype(jnp.bfloat16), expert_out)


def solution(mesh):
    return jax.shard_map(
        on_device,
        mesh=mesh,
        in_specs=(
            P(("ep", "tp"), None),
            P(("ep", "tp"), None),
            P(),
            P(None, "tp"),
            P(None, "tp"),
            P(None, "tp"),
            P(),
            P(None, "tp"),
            P(),
            P("ep", None),
            P("ep", None),
            P("ep", None, "tp"),
            P("ep", None, "tp"),
            P("ep", None, "tp"),
        ),
        out_specs=(P("ep", "tp"), P("ep", "tp")),
        check_vma=False,
    )
```

```python
import functools

import jax
import jax.numpy as jnp
from jax import lax
from jax.experimental import pallas as pl
from jax.experimental.pallas import tpu as pltpu
from jax.sharding import PartitionSpec as P


norm_eps = 1e-06


def rms_rows(values, gain_row):
    wide = values.astype(jnp.float32)
    scale = lax.rsqrt(jnp.mean(wide * wide, axis=-1, keepdims=True) + norm_eps)
    return (wide * scale * gain_row).astype(jnp.bfloat16)


def swapped(value, axis, mask):
    count = lax.axis_size(axis)
    return lax.ppermute(value, axis, [(source, source ^ mask) for source in range(count)])


def after(value, *earlier):
    return lax.optimization_barrier((value, earlier))[0]


def slot_masks(block_ids, labels, slot_cap):
    rows = block_ids.shape[1]
    hits = block_ids[:, None, :] == labels[None, :, None]
    member = jnp.any(hits, axis=0)
    order = jnp.arange(rows, dtype=jnp.int32)
    before = (order[:, None] < order[None, :]).astype(jnp.bfloat16)
    rank = jnp.dot(member.astype(jnp.bfloat16), before, preferred_element_type=jnp.float32)
    rank = jnp.where(member, rank, -1.0)
    slots = jnp.arange(slot_cap, dtype=jnp.int32).astype(jnp.float32)
    return hits, rank[:, None, :] == slots[None, :, None]


def swaps_direct(count):
    return count <= 16 and count & (count - 1) == 0


def start_order(count):
    across = [k for k in range(1, count) if k & (count // 2)]
    nearer = [k for k in range(2, count // 2)]
    half = len(across) // 2
    return across[:half] + [1] * (count > 2) + nearer + across[half:]


def exchange(chunks, axis, direct):
    if direct:
        moved = dict(chunks)
        for k in start_order(lax.axis_size(axis)):
            if k in chunks:
                moved[k] = swapped(chunks[k], axis, k)
        return moved
    rows = chunks[0]
    split = rows.reshape(lax.axis_size(axis), -1, rows.shape[1])
    moved = lax.all_to_all(split, axis, split_axis=0, concat_axis=0, tiled=True)
    return {0: moved.reshape(rows.shape)}


MIB = 1 << 20
STREAMS = 4
ANY = pl.BlockSpec(memory_space=pl.ANY)
VMEM = pl.BlockSpec(memory_space=pltpu.VMEM)
SMEM = pl.BlockSpec(memory_space=pltpu.SMEM)


def dispatch_kernel(direct, slot_cap, place_ref, ids_ref, source_ref, gain_ref, *refs):
    out_refs, (rows_ref, sem) = refs[:-2], refs[-2:]
    load = pltpu.make_async_copy(source_ref, rows_ref, sem)
    load.start()
    tok, width = rows_ref.shape
    total = ids_ref.shape[1]
    slots = sum(ref.shape[0] for ref in out_refs)
    experts = slots // slot_cap
    lanes = min(total, -(-tok // 128) * 128)
    tp_index, ep_index = place_ref[0], place_ref[1]
    ids = pltpu.roll(ids_ref[...], lax.rem(total - tp_index * tok, total), 1)[:, :lanes]
    labels = lax.broadcasted_iota(jnp.int32, (experts, lanes), 0)
    if direct:
        labels = labels ^ ep_index
    member = ids[0:1] == labels
    for pick in range(1, ids_ref.shape[0]):
        member = member | (ids[pick : pick + 1] == labels)
    first = lax.broadcasted_iota(jnp.int32, (lanes, lanes), 0)
    second = lax.broadcasted_iota(jnp.int32, (lanes, lanes), 1)
    before = jnp.where(first < second, 1.0, 0.0).astype(jnp.bfloat16)
    member = jnp.where(member, 1.0, 0.0)
    rank = jnp.dot(member.astype(jnp.bfloat16), before, preferred_element_type=jnp.float32)
    rank = jnp.where(member > 0.5, rank, -1.0).astype(jnp.bfloat16)
    slot = lax.broadcasted_iota(jnp.int32, (slots, experts), 0)
    start = lax.broadcasted_iota(jnp.int32, (slots, experts), 1) * slot_cap
    inside = (slot >= start) & (slot < start + slot_cap)
    spread = jnp.where(inside, 1.0, 0.0)
    rank_of = jnp.dot(spread.astype(jnp.bfloat16), rank, preferred_element_type=jnp.float32)
    offset = jnp.where(inside, (slot - start).astype(jnp.float32), 0.0)
    offset = jnp.sum(offset, axis=1, keepdims=True)
    mask = jnp.where(rank_of == offset, 1.0, 0.0)[:, :tok].astype(jnp.bfloat16)
    load.wait()
    wide = rows_ref[...].astype(jnp.float32)
    scale = lax.rsqrt(jnp.mean(wide * wide, axis=-1, keepdims=True) + norm_eps)
    normed = (wide * scale * gain_ref[...]).astype(jnp.bfloat16)
    step = min(width, 512)
    for col in range(0, width, step):
        part = jnp.dot(mask, normed[:, col : col + step], preferred_element_type=jnp.float32)
        part = part.astype(jnp.bfloat16)
        row = 0
        for ref in out_refs:
            ref[:, col : col + step] = part[row : row + ref.shape[0]]
            row += ref.shape[0]


def dispatched(place, ids, rows, gain, sizes, direct, slot_cap):
    width = rows.shape[1]
    return pl.pallas_call(
        functools.partial(dispatch_kernel, direct, slot_cap),
        out_shape=[pltpu.HBM((sizes[0], width), jnp.bfloat16)]
        + [pltpu.VMEM((size, width), jnp.bfloat16) for size in sizes[1:]],
        in_specs=[SMEM, VMEM, ANY, VMEM],
        out_specs=[VMEM] * len(sizes),
        scratch_shapes=[pltpu.VMEM(rows.shape, rows.dtype), pltpu.SemaphoreType.DMA],
        compiler_params=pltpu.CompilerParams(vmem_limit_bytes=56 * MIB),
        cost_estimate=pl.CostEstimate(
            flops=2 * sum(sizes) * rows.shape[0] * width, bytes_accessed=2 * MIB, transcendentals=0
        ),
        name="dispatch",
    )(place, ids, rows, gain)


def stream_hidden(row_refs, weight_refs, rows, weights, row_sems, weight_sems, later=()):
    chunks = row_sems.shape[0]
    depth = rows.shape[1] // chunks
    plan = []
    for chunk in range(chunks):
        part = pl.ds(chunk * depth, depth)
        copies, row = [], 0
        for index, ref in enumerate(row_refs):
            target = rows.at[pl.ds(row, ref.shape[0]), part]
            sem = row_sems.at[chunk, index]
            copies.append(pltpu.make_async_copy(ref.at[:, part], target, sem))
            row += ref.shape[0]
        for index, ref in enumerate(weight_refs):
            width = ref.shape[1]
            target = weights.at[index % 2, part, pl.ds(index // 2 * width, width)]
            sem = weight_sems.at[chunk, index]
            copies.append(pltpu.make_async_copy(ref.at[part, :], target, sem))
        for copy in copies:
            copy.start()
        plan.append(copies)
    gate_pre = up_pre = None
    for chunk in range(chunks):
        for copy in plan[chunk]:
            copy.wait()
        if chunk == 0:
            for copy in later:
                copy.start()
        part = slice(chunk * depth, (chunk + 1) * depth)
        here = rows[:, part]
        gate_term = jnp.dot(here, weights[0, part, :], preferred_element_type=jnp.float32)
        up_term = jnp.dot(here, weights[1, part, :], preferred_element_type=jnp.float32)
        gate_pre = gate_term if gate_pre is None else gate_pre + gate_term
        up_pre = up_term if up_pre is None else up_pre + up_term
    return (gate_pre / (1.0 + jnp.exp(-gate_pre)) * up_pre).astype(jnp.bfloat16)


def hidden_scratch(row_parts, weights):
    rows = sum(part.shape[0] for part in row_parts)
    depth, width = weights[0].shape
    return [
        pltpu.VMEM((rows, depth), jnp.bfloat16),
        pltpu.VMEM((2, depth, width * len(weights) // 2), jnp.bfloat16),
        pltpu.SemaphoreType.DMA((STREAMS, len(row_parts))),
        pltpu.SemaphoreType.DMA((STREAMS, len(weights))),
    ]


def hidden_cost(row_parts, weights):
    rows = sum(part.shape[0] for part in row_parts)
    depth, width = weights[0].shape
    return pl.CostEstimate(
        flops=2 * rows * depth * width * len(weights),
        bytes_accessed=2 * (rows * depth + len(weights) * depth * width),
        transcendentals=rows * width * len(weights) // 2,
    )


def first_kernel(row_count, *refs):
    row_refs, refs = refs[:row_count], refs[row_count:]
    weight_refs, (out_ref, *scratch) = refs[:-5], refs[-5:]
    out_ref[...] = stream_hidden(row_refs, weight_refs, *scratch)


def first_hidden(row_parts, weights):
    rows = sum(part.shape[0] for part in row_parts)
    width = weights[0].shape[1] * len(weights) // 2
    return pl.pallas_call(
        functools.partial(first_kernel, len(row_parts)),
        out_shape=pltpu.VMEM((rows, width), jnp.bfloat16),
        in_specs=[ANY] * (len(row_parts) + len(weights)),
        out_specs=VMEM,
        scratch_shapes=hidden_scratch(row_parts, weights),
        compiler_params=pltpu.CompilerParams(vmem_limit_bytes=56 * MIB),
        cost_estimate=hidden_cost(row_parts, weights),
        name="first_hidden",
    )(*row_parts, *weights)


def down_rows(place, first, second, weight_ref):
    half = first.shape[1] // 2
    total = None
    for j in range(4):
        source = first if j < 2 else second
        block = source[:, (j % 2) * half : (j % 2 + 1) * half]
        start = pl.multiple_of((place ^ j) * half, half)
        term = jnp.dot(block, weight_ref[pl.ds(start, half), :], preferred_element_type=jnp.float32)
        total = term if total is None else total + term
    return total.astype(jnp.bfloat16)


def second_kernel(row_count, weight_count, early_rows, place_ref, first_ref, *refs):
    row_refs, refs = refs[:row_count], refs[row_count:]
    weight_refs, refs = refs[:weight_count], refs[weight_count:]
    down_refs, (hidden_ref, *refs) = refs[:2], refs[2:]
    out_refs, (first_rows, down_own, down_near, down_sems, *scratch) = refs[:-8], refs[-8:]
    sources, targets = (first_ref, *down_refs), (first_rows, down_own, down_near)
    loads = [
        pltpu.make_async_copy(ref, target, down_sems.at[index])
        for index, (ref, target) in enumerate(zip(sources, targets))
    ]
    hidden_ref[...] = stream_hidden(row_refs, weight_refs, *scratch, later=loads)
    loads[0].wait()
    first = first_rows[early_rows:]
    second = hidden_ref[early_rows:]
    col = 0
    for load, weight in zip(loads[1:], (down_own, down_near)):
        load.wait()
        total = down_rows(place_ref[0], first, second, weight)
        row = 0
        for ref in out_refs:
            ref[:, col : col + total.shape[1]] = total[row : row + ref.shape[0]]
            row += ref.shape[0]
        col += total.shape[1]


def second_hidden(place, first, row_parts, weights, downs, sizes, early):
    rows = sum(sizes)
    width = weights[0].shape[1] * len(weights) // 2
    out_width = 2 * downs[0].shape[1]
    outs = [pltpu.VMEM((rows, width), jnp.bfloat16)]
    outs += [pltpu.VMEM((sizes[k], out_width), jnp.bfloat16) for k in early]
    hidden, *results = pl.pallas_call(
        functools.partial(second_kernel, len(row_parts), len(weights), sum(sizes[: early[0]])),
        out_shape=outs,
        in_specs=[SMEM, ANY] + [ANY] * (len(row_parts) + len(weights) + 2),
        out_specs=[VMEM] * len(outs),
        scratch_shapes=[
            pltpu.VMEM(first.shape, jnp.bfloat16),
            pltpu.VMEM(downs[0].shape, jnp.bfloat16),
            pltpu.VMEM(downs[1].shape, jnp.bfloat16),
            pltpu.SemaphoreType.DMA((3,)),
        ]
        + hidden_scratch(row_parts, weights),
        compiler_params=pltpu.CompilerParams(vmem_limit_bytes=56 * MIB),
        cost_estimate=pl.CostEstimate(flops=MIB, bytes_accessed=MIB, transcendentals=0),
        name="second_hidden",
    )(place, first, *row_parts, *weights, *downs)
    return hidden, dict(zip(early, results))


def late_kernel(far, sizes, early, place_ref, *refs):
    first_ref, second_ref, first_far_ref, second_far_ref, own_ref, near_ref, *refs = refs
    out_refs, (down_own, down_near, sems) = refs[:-3], refs[-3:]
    loads = [
        pltpu.make_async_copy(own_ref, down_own, sems.at[0]),
        pltpu.make_async_copy(near_ref, down_near, sems.at[1]),
    ]
    for load in loads:
        load.start()
    later = [k for k in range(len(sizes)) if k not in early]
    own_rows = sum(sizes[k] for k in later)
    col = 0
    for load, weight_ref in zip(loads, (down_own, down_near)):
        load.wait()
        total = down_rows(place_ref[0] ^ far, first_far_ref[...], second_far_ref[...], weight_ref)
        width = total.shape[1]
        row = 0
        for k, ref in enumerate(out_refs):
            at = 0 if k in early else sizes[k]
            ref[at:, col : col + width] = total[row : row + sizes[k]]
            row += sizes[k]
        if later:
            total = down_rows(place_ref[0], first_ref[:own_rows], second_ref[:own_rows], weight_ref)
            row = 0
            for k in later:
                out_refs[k][: sizes[k], col : col + width] = total[row : row + sizes[k]]
                row += sizes[k]
        col += width


def late_results(place, far, hidden_parts, downs, sizes, early):
    out_width = 2 * downs[0].shape[1]
    rows = [sizes[k] if k in early else 2 * sizes[k] for k in range(len(sizes))]
    return pl.pallas_call(
        functools.partial(late_kernel, far, tuple(sizes), tuple(early)),
        out_shape=[pltpu.HBM((count, out_width), jnp.bfloat16) for count in rows],
        in_specs=[SMEM] + [VMEM] * 4 + [ANY] * 2,
        out_specs=[VMEM] * len(rows),
        scratch_shapes=[
            pltpu.VMEM(downs[0].shape, jnp.bfloat16),
            pltpu.VMEM(downs[1].shape, jnp.bfloat16),
            pltpu.SemaphoreType.DMA((2,)),
        ],
        compiler_params=pltpu.CompilerParams(vmem_limit_bytes=24 * MIB),
        cost_estimate=pl.CostEstimate(
            flops=2 * sum(rows) * downs[0].shape[0] * out_width,
            bytes_accessed=4 * MIB,
            transcendentals=0,
        ),
        name="late_down",
    )(place, *hidden_parts, *downs)


def front_kernel(place_ref, *refs):
    part_refs, weight_refs, refs = refs[:4], refs[4:7], refs[7:]
    product_ref, gate_ref, rim_ref, rows, weights, row_sems, weight_sems = refs
    tok = part_refs[0].shape[0]
    copies = []
    for j, ref in enumerate(part_refs):
        start = pl.multiple_of((place_ref[0] ^ j) * tok, tok)
        copies.append(pltpu.make_async_copy(ref, rows.at[pl.ds(start, tok)], row_sems.at[j]))
    loads = [
        pltpu.make_async_copy(ref, weights.at[index], weight_sems.at[index])
        for index, ref in enumerate(weight_refs)
    ]
    for copy in copies + loads[:1]:
        copy.start()
    for copy in copies:
        copy.wait()
    loads[1].start()
    loads[0].wait()
    loads[2].start()
    in_gate = jnp.dot(rows[...], weights[0], preferred_element_type=jnp.float32)
    loads[1].wait()
    values = jnp.dot(rows[...], weights[1], preferred_element_type=jnp.float32)
    product = (in_gate * values).astype(jnp.bfloat16)
    product_ref[...] = product
    rim_ref[...] = product[product.shape[0] - rim_ref.shape[0] :]
    loads[2].wait()
    gate_ref[...] = jnp.dot(rows[...], weights[2], preferred_element_type=jnp.float32)


def mixer_front(place, parts, weights, rim):
    rows = sum(part.shape[0] for part in parts)
    depth, width = weights[0].shape
    return pl.pallas_call(
        front_kernel,
        out_shape=[
            pltpu.VMEM((rows, width), jnp.bfloat16),
            pltpu.VMEM((rows, width), jnp.float32),
            pltpu.VMEM((rim, width), jnp.bfloat16),
        ],
        in_specs=[SMEM] + [ANY] * 7,
        out_specs=[VMEM, VMEM, VMEM],
        scratch_shapes=[
            pltpu.VMEM((rows, depth), jnp.bfloat16),
            pltpu.VMEM((3, depth, width), jnp.bfloat16),
            pltpu.SemaphoreType.DMA((4,)),
            pltpu.SemaphoreType.DMA((3,)),
        ],
        compiler_params=pltpu.CompilerParams(vmem_limit_bytes=56 * MIB),
        cost_estimate=pl.CostEstimate(
            flops=6 * rows * depth * width, bytes_accessed=8 * MIB, transcendentals=0
        ),
        name="mixer_front",
    )(place, *parts, *weights)


def share_masks(mask, hits, share_rows):
    share_of = jnp.sum(jnp.where(hits, share_rows[:, None, :], 0.0), axis=0)
    mixed = jnp.where(mask, share_of[:, None, :], 0.0).reshape(-1, mask.shape[2])
    high = mixed.astype(jnp.bfloat16)
    return high, (mixed - high.astype(jnp.float32)).astype(jnp.bfloat16)


def combine_rows(masks, returned):
    dims = (((0,), (0,)), ((), ()))
    total = lax.dot_general(masks[0], returned, dims, preferred_element_type=jnp.float32)
    total = total + lax.dot_general(masks[1], returned, dims, preferred_element_type=jnp.float32)
    return total


def on_device(
    mixer_in,
    expert_in,
    mixer_gain,
    in_gate_weight,
    out_gate_weight,
    value_weight,
    conv_taps,
    mixer_proj,
    expert_gain,
    route_ids,
    route_weights,
    gate_weight,
    up_weight,
    down_weight,
):
    tok_dev = mixer_in.shape[0]
    tp_count = lax.axis_size("tp")
    ep_count = lax.axis_size("ep")
    top_count = route_ids.shape[1]
    experts = ep_count * gate_weight.shape[0]
    slot_cap = max(2, 2 * tok_dev * top_count // experts)
    tp_index = lax.axis_index("tp")
    ep_index = lax.axis_index("ep")
    direct = swaps_direct(ep_count)
    near, far = 1, tp_count // 2

    gates, ups = {0: gate_weight[0]}, {0: up_weight[0]}
    gates[far] = swapped(gates[0], "tp", far)
    ups[far] = swapped(ups[0], "tp", far)
    gates[near] = swapped(gates[0], "tp", near)
    ups[near] = swapped(ups[0], "tp", near)
    down_own = down_weight[0]
    down_near = swapped(down_own, "tp", near)
    order = [0, near, far, far ^ near]

    def rows_of(weight, j, width):
        return lax.dynamic_slice_in_dim(weight, (tp_index ^ j) * width, width, 0)

    peers = jnp.arange(experts, dtype=jnp.int32)
    labels = (peers ^ ep_index) if direct else peers

    def block_of(values, j):
        return lax.dynamic_slice_in_dim(values, (tp_index ^ j) * tok_dev, tok_dev, 0)

    hits_own, mask_own = slot_masks(block_of(route_ids, 0).T, labels, slot_cap)
    hits_far, mask_far = slot_masks(block_of(route_ids, far).T, labels, slot_cap)
    shares = route_weights / jnp.sum(route_weights, axis=1, keepdims=True)
    masks_own = share_masks(mask_own, hits_own, block_of(shares, 0).T)
    masks_far = share_masks(mask_far, hits_far, block_of(shares, far).T)
    chan_width = in_gate_weight.shape[1]
    tap_count = conv_taps.shape[0]
    tap_rows = lax.dynamic_slice_in_dim(conv_taps, tp_index * chan_width, chan_width, 1)
    tap_rows = [tap_rows[tap_index] for tap_index in range(tap_count)]
    mixer_normed = rms_rows(mixer_in, mixer_gain)
    place = jnp.where(jnp.arange(2) == 0, tp_index, ep_index).astype(jnp.int32)
    sizes = [slot_cap] * experts if direct else [experts * slot_cap]
    early = list(range(len(sizes) // 2, len(sizes)))
    outgoing = dispatched(
        place, route_ids.T, expert_in, expert_gain[None, :], sizes, direct, slot_cap
    )
    arrived = exchange(dict(enumerate(outgoing)), "ep", direct)
    gates[far ^ near] = swapped(gates[far], "tp", near)
    ready = (masks_own, masks_far, mixer_normed, gates[far ^ near])
    ready += (gates[near], ups[near], down_near)
    ready += tuple(tap_rows)
    arrived[0] = after(arrived[0], *ready)
    slots_in = [arrived[k] for k in range(len(sizes))]

    first = first_hidden(slots_in, [half[j] for j in (0, near) for half in (gates, ups)])
    ups[far ^ near] = swapped(after(ups[far], first), "tp", near)
    downs = (down_own, down_near)
    second, done_own = second_hidden(
        place,
        first,
        slots_in,
        [half[j] for j in (far, far ^ near) for half in (gates, ups)],
        downs,
        sizes,
        early,
    )
    first_far = swapped(after(first, ups[far]), "tp", far)
    second_far = swapped(second, "tp", far)
    back_own = exchange(done_own, "ep", direct)

    normed = {0: mixer_normed}
    normed[far] = swapped(normed[0], "tp", far)
    normed[near] = swapped(normed[0], "tp", near)
    normed = {j: after(normed[j], second) for j in normed}
    normed[far ^ near] = swapped(normed[far], "tp", near)
    front_weights = [in_gate_weight, value_weight, out_gate_weight]
    product, out_gate, rim_sent = mixer_front(
        place, [normed[j] for j in order], front_weights, tap_count - 1
    )
    row_count = product.shape[0]
    steps = [(source, source + 1) for source in range(ep_count - 1)]
    rim_rows = lax.ppermute(rim_sent, "ep", steps)
    extended = jnp.concatenate([rim_rows, product], axis=0).astype(jnp.float32)
    conv_sum = tap_rows[0] * extended[0:row_count]
    for tap_index in range(1, tap_count):
        conv_sum = conv_sum + tap_rows[tap_index] * extended[tap_index : tap_index + row_count]
    gated = {0: (out_gate * conv_sum).astype(jnp.bfloat16)}
    gated[far] = swapped(gated[0], "tp", far)
    gated[near] = swapped(gated[0], "tp", near)
    gated[far ^ near] = swapped(gated[far], "tp", near)
    mixer_sum = None
    for j in order:
        term = jnp.dot(
            gated[j], rows_of(mixer_proj, j, chan_width), preferred_element_type=jnp.float32
        )
        mixer_sum = term if mixer_sum is None else mixer_sum + term
    first_far = after(first_far, product)
    late = late_results(place, far, (first, second, first_far, second_far), downs, sizes, early)
    back_late = exchange(dict(enumerate(late)), "ep", direct)
    width = slot_cap if direct else sizes[0]
    later = [k for k in range(len(sizes)) if k not in early]
    own_early = combine_rows(
        [mask[early[0] * width :] for mask in masks_own],
        jnp.concatenate([back_own[k] for k in early], axis=0),
    )
    back_late[0] = after(back_late[0], mixer_sum, own_early)
    far_rows = [back_late[k][-sizes[k] :] for k in range(len(sizes))]
    mixed_own = own_early
    if later:
        own_rows = [back_late[k][: sizes[k]] for k in later]
        masks_later = [mask[: len(later) * width] for mask in masks_own]
        mixed_own = mixed_own + combine_rows(masks_later, jnp.concatenate(own_rows, axis=0))
    mixed_own = mixed_own.astype(jnp.bfloat16)
    mixed_far = combine_rows(masks_far, jnp.concatenate(far_rows, axis=0)).astype(jnp.bfloat16)
    mixed = jnp.concatenate([mixed_own, mixed_far], axis=0)
    col_width = down_own.shape[1]
    mixed_near = swapped(mixed[:, col_width:], "tp", near)
    expert_out = jnp.zeros((tp_count * tok_dev, col_width), jnp.bfloat16)
    for j, block in (
        (0, mixed[:tok_dev, :col_width]),
        (far, mixed[tok_dev:, :col_width]),
        (near, mixed_near[:tok_dev]),
        (far ^ near, mixed_near[tok_dev:]),
    ):
        expert_out = lax.dynamic_update_slice_in_dim(
            expert_out, block, (tp_index ^ j) * tok_dev, 0
        )

    return (mixer_sum.astype(jnp.bfloat16), expert_out)


def solution(mesh):
    return jax.shard_map(
        on_device,
        mesh=mesh,
        in_specs=(
            P(("ep", "tp"), None),
            P(("ep", "tp"), None),
            P(),
            P(None, "tp"),
            P(None, "tp"),
            P(None, "tp"),
            P(),
            P(None, "tp"),
            P(),
            P("ep", None),
            P("ep", None),
            P("ep", None, "tp"),
            P("ep", None, "tp"),
            P("ep", None, "tp"),
        ),
        out_specs=(P("ep", "tp"), P("ep", "tp")),
        check_vma=False,
    )
```
